32 devices in a mesh: gr: 2 (over x), sp: 8 (over z, y), tp: 2 (over core).
Axes of the slice: x: 2, y: 2, z: 4, core: 2. Of those that a mesh axis runs over, the one named last changes fastest.
Arguments:
- tokens: bfloat16 [2, 2, 6144, 2048], P('gr', 'tp', 'sp'), may hold values from -6 to 6
- key_weight: bfloat16 [2048, 2048], replicated, may hold values from -0.125 to 0.125
- value_weight: bfloat16 [2048, 2048], replicated, may hold values from -0.125 to 0.125
- cum_gate: float32 [2, 32, 2, 6144], P('gr', None, 'tp', 'sp'), may hold values from -12588 to 0, as said below
- query: bfloat16 [2, 32, 64], P('gr', 'sp'), may hold values from -12 to 12
Outputs:
- kv_cache: bfloat16 [2, 32, 12288, 128], P('gr', 'sp', 'tp')
- gate_cache: float32 [2, 32, 12288], P('gr', 'sp', 'tp')
- read: bfloat16 [2, 32, 64], P('gr', 'sp')
The draws below stay inside these ranges and needn't reach their ends.
Inputs may be any that keep to these rules, and one draw needn't show every extreme that they name: `cum_gate`: each head's entries never rise along the positions.
All inputs are finite; a program needn't handle non-finite values.
Results may differ from the reference program's by a relative error of at most 0.012.
Values may be sent and summed in bfloat16 or wider, within the bound.
A program may use at most 128 MiB of HBM per device.

```python
import jax
import jax.numpy as jnp

D = 2048
HEADS = 32
HD = 64
TOK_DEV = 768
SPAN = 6144
LEN = 12288
BATCH = 2
N_TP = 2


def draw_cum_gate(key, part):
    keys = jax.random.split(jax.random.fold_in(key, 7), 5)
    fast = jax.random.randint(keys[0], (BATCH, HEADS, 1), 0, 2) == 1
    spread = jnp.exp(jax.random.uniform(keys[1], (BATCH, HEADS, 1), jnp.float32, -0.7, 0.7))
    rate = jnp.where(fast, spread / 40.0, spread / LEN)
    blocks = LEN // TOK_DEV
    factor = jnp.exp(jax.random.uniform(keys[2], (BATCH, HEADS, blocks, 1), jnp.float32, -0.85, 0.85))
    factor = jnp.broadcast_to(factor, (BATCH, HEADS, blocks, TOK_DEV)).reshape(BATCH, HEADS, LEN)
    rough = jax.random.uniform(keys[3], (BATCH, HEADS, LEN), jnp.float32, 0.5, 1.5)
    log_gate = -rate * factor * rough
    start = -jax.random.uniform(keys[4], (BATCH, HEADS, 1), jnp.float32, 0.0, 300.0)
    total = start + jnp.cumsum(log_gate, axis=-1)
    return total.reshape(BATCH, HEADS, N_TP, SPAN).astype(jnp.float32)


def steps_of(key, shape, cuts, smallest, largest):
    factor_of, own = 1.0, jax.random.fold_in(key, 6)
    for axis_at, blocks in cuts:
        steps = jnp.exp(jax.random.uniform(jax.random.fold_in(own, axis_at), (blocks,), jnp.float32, smallest / len(cuts), largest / len(cuts)))
        factor_of = factor_of * jnp.repeat(steps, shape[axis_at] // blocks).reshape([-1 if axis == axis_at else 1 for axis in range(len(shape))])
    return factor_of


def normal_values(key, shape, scale, most, pieces=(), held_as=jnp.bfloat16):
    values = jax.random.normal(key, shape, jnp.float32) * scale
    if len(pieces) > 0:
        values = steps_of(key, shape, pieces, -0.22, 0.18) * values
    return jnp.clip(values, min=-most, max=most).astype(held_as)


def setup_inputs(seed: int = 0) -> dict:
    key_of = jax.random.split(jax.random.key(seed), 6)
    tokens = normal_values(key_of[0], (BATCH, N_TP, SPAN, D), 1.0, 6.0, ((0, 2), (1, 2), (2, 8)))
    key_weight = normal_values(key_of[1], (D, HEADS * HD), D ** -0.5, 0.125)
    value_weight = normal_values(key_of[2], (D, HEADS * HD), D ** -0.5, 0.125)
    cum_gate = draw_cum_gate(jax.random.fold_in(key_of[5], 71), 0)
    query = normal_values(key_of[4], (BATCH, HEADS, HD), 3.0, 12.0, ((0, 2), (1, 8)))
    return dict(tokens=tokens, key_weight=key_weight, value_weight=value_weight, cum_gate=cum_gate, query=query)


def reference(tokens, key_weight, value_weight, cum_gate, query):
    count = tokens.shape[0]
    rows = tokens.reshape(count * LEN, D)

    def project(weight):
        out = jnp.dot(rows, weight, preferred_element_type=jnp.float32).astype(jnp.bfloat16)
        return jnp.transpose(out.reshape(count, LEN, HEADS, HD), (0, 2, 1, 3))

    keys = project(key_weight)
    values = project(value_weight)
    kv_cache = jnp.concatenate([keys, values], axis=-1)
    gate_cache = cum_gate.reshape(count, HEADS, LEN)
    scores = jnp.einsum("bhe,bhse->bhs", query.astype(jnp.float32), keys.astype(jnp.float32))
    scores = scores * (HD ** -0.5) - gate_cache
    top = jnp.max(scores, axis=-1, keepdims=True)
    weights = jnp.exp(scores - top)
    total = jnp.sum(weights, axis=-1)
    probs = weights.astype(jnp.bfloat16).astype(jnp.float32)
    weighted = jnp.einsum("bhs,bhse->bhe", probs, values.astype(jnp.float32))
    read = (weighted / total[..., None]).astype(jnp.bfloat16)
    return kv_cache, gate_cache, read
```

```python
import functools

import jax
import jax.numpy as jnp
from jax import lax
from jax.experimental import pallas as pl
from jax.experimental.pallas import tpu as pltpu
from jax.sharding import PartitionSpec as P

MESH = pl.DeviceIdType.MESH
LANES = 128


def partner(step, me, n):
    if n % 2:
        return lax.rem(me + 1 + step, n)
    turn, flip = step // 2, lax.rem(step, 2)
    flip = jnp.where(turn == n // 2 - 1, 1 - flip, flip)
    return lax.rem(me // 2 + 1 + turn, n // 2) * 2 + lax.rem(me + flip, 2)


def exchange_kernel(
    n, per_owner, tile, head,
    tokens, key_weight, value_weight, gates, query,
    kv, gate_out, read,
    rows, weights, outgoing, gate_own, gate_send, gate_in, query_own, query_in, part_send, part_in, mine, theirs,
    row_sem, weight_sem, small_sem, send_sem, recv_sem,
    gate_sent, gate_recv, query_sent, query_recv, part_sent, part_recv, pair_sem,
):
    me = lax.axis_index("sp")
    core = lax.axis_index("tp")
    count = rows.shape[0]
    tiles = count // tile
    early = max(tiles - 1, 1)
    columns = weights.shape[3]
    group_heads = columns // head
    owners = group_heads // per_owner
    groups = n // owners

    def group_of(step):
        if owners == 1:
            return partner(step, me, n)
        return lax.rem(me // owners + 1 + step, groups)

    def load_rows(t):
        span = pl.ds(t * tile, tile)
        return pltpu.make_async_copy(tokens.at[span, :], rows.at[span, :], row_sem.at[t])

    def load_weight(step, which):
        at = pl.ds(pl.multiple_of(group_of(step) * columns, columns), columns)
        source = (key_weight, value_weight)[which]
        return pltpu.make_async_copy(
            source.at[:, at], weights.at[step, which], weight_sem.at[step, which]
        )

    load_query = pltpu.make_async_copy(query, query_own, small_sem.at[0])
    load_gates = pltpu.make_async_copy(gates, gate_own, small_sem.at[1])
    load_query.start()
    load_rows(0).start()
    load_weight(0, 0).start()
    load_weight(0, 1).start()
    load_gates.start()
    for t in range(1, tiles):
        load_rows(t).start()

    barrier = pltpu.get_barrier_semaphore()

    @pl.loop(1, n)
    def _(k):
        pl.semaphore_signal(
            barrier, inc=1, device_id={"sp": lax.rem(me + k, n)}, device_id_type=MESH
        )

    pl.semaphore_signal(barrier, inc=1, device_id={"tp": 1 - core}, device_id_type=MESH)

    load_query.wait()
    wide = jnp.concatenate(
        [query_own[...].astype(jnp.float32), jnp.zeros((per_owner, LANES - head), jnp.float32)], axis=1
    ) * (head ** -0.5)
    query_in[me] = wide

    def query_copy(owner):
        return pltpu.make_async_remote_copy(
            src_ref=query_in.at[me], dst_ref=query_in.at[me],
            send_sem=query_sent.at[owner], recv_sem=query_recv.at[me],
            device_id={"sp": owner}, device_id_type=MESH,
        )

    def gate_copy(owner):
        return pltpu.make_async_remote_copy(
            src_ref=gate_send.at[owner], dst_ref=gate_in.at[me],
            send_sem=gate_sent.at[owner], recv_sem=gate_recv.at[me],
            device_id={"sp": owner}, device_id_type=MESH,
        )

    def part_copy(owner):
        return pltpu.make_async_remote_copy(
            src_ref=part_send.at[owner], dst_ref=part_in.at[me],
            send_sem=part_sent.at[owner], recv_sem=part_recv.at[me],
            device_id={"sp": owner}, device_id_type=MESH,
        )

    def block_copy(owner, t):
        return pltpu.make_async_remote_copy(
            src_ref=outgoing.at[owner, :, pl.ds(t * tile, tile), :],
            dst_ref=kv.at[:, pl.ds(pl.multiple_of(me * count + t * tile, tile), tile), :],
            send_sem=send_sem.at[owner, t], recv_sem=recv_sem.at[me, t],
            device_id={"sp": owner}, device_id_type=MESH,
        )

    def block_own(t):
        return pltpu.make_async_copy(
            outgoing.at[me, :, pl.ds(t * tile, tile), :],
            kv.at[:, pl.ds(pl.multiple_of(me * count + t * tile, tile), tile), :],
            recv_sem.at[me, t],
        )

    def send_block(owner, t):
        @pl.when(owner != me)
        def _():
            block_copy(owner, t).start()

        @pl.when(owner == me)
        def _():
            block_own(t).start()

    def own_gates(owner, span):
        return jnp.concatenate([gate_own[owner, h, :, span] for h in range(per_owner)], axis=0)

    low = lax.broadcasted_iota(jnp.int32, (tile, LANES), 1) < head

    def open_links():
        load_gates.wait()

        @pl.loop(0, n)
        def _(k):
            gate_send[k] = own_gates(k, slice(None)).astype(jnp.bfloat16)

        gate_in[me] = own_gates(me, slice(None)).astype(jnp.bfloat16)
        pl.semaphore_wait(barrier, n)

        @pl.loop(0, n - 1)
        def _(k):
            owner = partner(k, me, n)
            gate_copy(owner).start()
            query_copy(owner).start()

    def project(step, first):
        group = group_of(step)

        if first:
            for ahead in range(1, min(3, groups)):
                load_weight(ahead, 0).start()
                load_weight(ahead, 1).start()
        else:
            @pl.when(step + 2 < groups)
            def _():
                load_weight(step + 2, 0).start()
                load_weight(step + 2, 1).start()

        load_weight(step, 0).wait()
        load_weight(step, 1).wait()
        for t in range(tiles):
            if first:
                load_rows(t).wait()
            left = rows[pl.ds(t * tile, tile), :]
            keys = jnp.dot(left, weights[step, 0], preferred_element_type=jnp.float32)
            values = jnp.dot(left, weights[step, 1], preferred_element_type=jnp.float32)
            for pair in range(columns // LANES):
                span = slice(pair * LANES, (pair + 1) * LANES)
                k, v = keys[:, span], values[:, span]
                joined = (
                    jnp.where(low, k, pltpu.roll(v, head, 1)),
                    jnp.where(low, pltpu.roll(k, head, 1), v),
                )
                for half in range(2):
                    local = pair * 2 + half
                    owner = group * owners + local // per_owner
                    outgoing[owner, local % per_owner, pl.ds(t * tile, tile), :] = joined[
                        half
                    ].astype(jnp.bfloat16)
            if first and t == 0:
                open_links()
            if t < early:
                for j in range(owners):
                    send_block(group * owners + j, t)

    project(0, True)

    def later(step, carry):
        project(step, False)
        return carry

    lax.fori_loop(1, groups, later, 0)

    @pl.loop(0, n - 1)
    def _(k):
        source = partner(k, me, n)
        query_copy(source).wait_send()
        pltpu.make_async_copy(query_in.at[source], query_in.at[source], query_recv.at[source]).wait()

    head_row = lax.broadcasted_iota(jnp.int32, (per_owner, LANES), 0)
    tile_row = lax.broadcasted_iota(jnp.int32, (per_owner, tile), 0)
    lane = lax.broadcasted_iota(jnp.int32, (per_owner, LANES), 1)

    def read_own(k, carry):
        owner = partner(k, me, n)
        asked = query_in[owner]
        queries = [
            jnp.where(head_row == h, asked, 0.0).astype(jnp.bfloat16) for h in range(per_owner)
        ]
        top = jnp.full((per_owner, 1), -1e30, jnp.float32)
        total = jnp.zeros((per_owner, 1), jnp.float32)
        weighted = jnp.zeros((per_owner, LANES), jnp.float32)
        for t in range(tiles):
            span = pl.ds(t * tile, tile)
            blocks = [outgoing[owner, h, span, :] for h in range(per_owner)]
            scores = None
            for h in range(per_owner):
                term = lax.dot_general(
                    queries[h], blocks[h], (((1,), (1,)), ((), ())), preferred_element_type=jnp.float32
                )
                scores = term if scores is None else scores + term
            scores = scores - own_gates(owner, span)
            new_top = jnp.maximum(top, jnp.max(scores, axis=1, keepdims=True))
            scale = jnp.exp(top - new_top)
            probs = jnp.exp(scores - new_top)
            total = total * scale + jnp.sum(probs, axis=1, keepdims=True)
            weighted = weighted * scale
            for h in range(per_owner):
                picked = jnp.where(tile_row == h, probs, 0.0).astype(jnp.bfloat16)
                weighted = weighted + jnp.dot(picked, blocks[h], preferred_element_type=jnp.float32)
            top = new_top
        packed = jnp.where(lane < head // 2, top, jnp.where(lane < head, total, weighted))
        part_send[owner] = packed

        @pl.when(owner != me)
        def _():
            part_copy(owner).start()

        return carry

    lax.fori_loop(0, n, read_own, 0)

    if early < tiles:
        @pl.loop(0, n)
        def _(k):
            owner = partner(k, me, n)
            for t in range(early, tiles):
                send_block(owner, t)

    @pl.loop(0, n - 1)
    def _(k):
        source = partner(k, me, n)
        gate_copy(source).wait_send()
        pltpu.make_async_copy(gate_in.at[source], gate_in.at[source], gate_recv.at[source]).wait()

    for source in range(n):
        gate_out[:, source * count:(source + 1) * count] = gate_in[source].astype(jnp.float32)

    def merge(one, two):
        top_one, top_two = one[:, :1], two[:, :1]
        joint = jnp.maximum(top_one, top_two)
        both = one * jnp.exp(top_one - joint) + two * jnp.exp(top_two - joint)
        return jnp.where(lane < head // 2, joint, both)

    def gather(k, carry):
        source = partner(k, me, n)
        part_copy(source).wait_send()
        pltpu.make_async_copy(part_in.at[source], part_in.at[source], part_recv.at[source]).wait()
        return merge(carry, part_in[source])

    packed = lax.fori_loop(0, n - 1, gather, part_send[me])
    mine[...] = packed
    swap = pltpu.make_async_remote_copy(
        src_ref=mine, dst_ref=theirs, send_sem=pair_sem.at[0], recv_sem=pair_sem.at[1],
        device_id={"tp": 1 - core}, device_id_type=MESH,
    )
    swap.start()
    swap.wait()
    other = theirs[...]
    joint = merge(jnp.where(core == 0, packed, other), jnp.where(core == 0, other, packed))
    at = head // 2
    answer = joint / joint[:, at:at + 1]
    read[...] = pltpu.roll(answer, head, 1)[:, :head].astype(jnp.bfloat16)

    for t in range(tiles):
        block_own(t).wait()

        @pl.loop(0, n - 1)
        def _(k, t=t):
            source = partner(n - 2 - k, me, n)
            block_copy(source, t).wait_send()
            pltpu.make_async_copy(
                kv.at[:, pl.ds(t * tile, tile), :], kv.at[:, pl.ds(t * tile, tile), :], recv_sem.at[source, t]
            ).wait()


def finish_kernel(pieces, kv, gates, answer, kv_out, gate_out, read, sem):
    heads, length = kv.shape[0], kv.shape[1]
    part = length // pieces
    copies = [
        pltpu.make_async_copy(
            kv.at[h, pl.ds(p * part, part), :], kv_out.at[h, pl.ds(p * part, part), :], sem.at[h * pieces + p]
        )
        for p in range(pieces)
        for h in range(heads)
    ]
    copies.append(pltpu.make_async_copy(gates, gate_out, sem.at[heads * pieces]))
    copies.append(pltpu.make_async_copy(answer, read, sem.at[heads * pieces + 1]))
    for copy in copies:
        copy.start()
    for copy in copies:
        copy.wait()


def on_device(n, tokens, key_weight, value_weight, cum_gate, query):
    _, _, count, width = tokens.shape
    heads = cum_gate.shape[1]
    per_owner, head = query.shape[1], query.shape[2]
    tile = 256 if count % 256 == 0 else count
    columns = max(per_owner * head, LANES)
    groups = heads * head // columns
    tiles = count // tile
    any_space = pl.BlockSpec(memory_space=pl.ANY)
    vmem = pl.BlockSpec(memory_space=pltpu.VMEM)
    kv, gates, answer = pl.pallas_call(
        functools.partial(exchange_kernel, n, per_owner, tile, head),
        name="exchange",
        out_shape=(
            pltpu.VMEM((per_owner, n * count, 2 * head), jnp.bfloat16),
            pltpu.VMEM((per_owner, n * count), jnp.float32),
            pltpu.VMEM((per_owner, head), jnp.bfloat16),
        ),
        in_specs=[any_space] * 5,
        out_specs=(vmem, vmem, vmem),
        scratch_shapes=[
            pltpu.VMEM((count, width), jnp.bfloat16),
            pltpu.VMEM((groups, 2, width, columns), jnp.bfloat16),
            pltpu.VMEM((n, per_owner, count, 2 * head), jnp.bfloat16),
            pltpu.VMEM((n, per_owner, 1, count), jnp.float32),
            pltpu.VMEM((n, per_owner, count), jnp.bfloat16),
            pltpu.VMEM((n, per_owner, count), jnp.bfloat16),
            pltpu.VMEM((per_owner, head), jnp.bfloat16),
            pltpu.VMEM((n, per_owner, LANES), jnp.float32),
            pltpu.VMEM((n, per_owner, LANES), jnp.float32),
            pltpu.VMEM((n, per_owner, LANES), jnp.float32),
            pltpu.VMEM((per_owner, LANES), jnp.float32),
            pltpu.VMEM((per_owner, LANES), jnp.float32),
            pltpu.SemaphoreType.DMA((tiles,)),
            pltpu.SemaphoreType.DMA((groups, 2)),
            pltpu.SemaphoreType.DMA((2,)),
            pltpu.SemaphoreType.DMA((n, tiles)),
            pltpu.SemaphoreType.DMA((n, tiles)),
            pltpu.SemaphoreType.DMA((n,)),
            pltpu.SemaphoreType.DMA((n,)),
            pltpu.SemaphoreType.DMA((n,)),
            pltpu.SemaphoreType.DMA((n,)),
            pltpu.SemaphoreType.DMA((n,)),
            pltpu.SemaphoreType.DMA((n,)),
            pltpu.SemaphoreType.DMA((2,)),
        ],
        compiler_params=pltpu.CompilerParams(
            collective_id=0, has_side_effects=True, vmem_limit_bytes=56 * 1024 * 1024
        ),
    )(
        tokens.reshape(count, width),
        key_weight,
        value_weight,
        cum_gate.reshape(n, per_owner, 1, count),
        query.reshape(per_owner, head),
    )
    pieces = 4 if n % 4 == 0 else 1
    kv_out, gate_out, read = pl.pallas_call(
        functools.partial(finish_kernel, pieces),
        name="finish",
        out_shape=(
            jax.ShapeDtypeStruct((per_owner, n * count, 2 * head), jnp.bfloat16),
            jax.ShapeDtypeStruct((per_owner, n * count), jnp.float32),
            jax.ShapeDtypeStruct((per_owner, head), jnp.bfloat16),
        ),
        in_specs=[vmem, vmem, vmem],
        out_specs=(any_space, any_space, any_space),
        scratch_shapes=[pltpu.SemaphoreType.DMA((per_owner * pieces + 2,))],
        compiler_params=pltpu.CompilerParams(vmem_limit_bytes=16 * 1024 * 1024),
    )(kv, gates, answer)
    return kv_out[None], gate_out[None], read[None]


def solution(mesh):
    placed = (P("gr", "tp", "sp", None), P(), P(), P("gr", None, "tp", "sp"), P("gr", "sp", None))
    return jax.shard_map(
        functools.partial(on_device, mesh.shape["sp"]),
        mesh=mesh,
        in_specs=placed,
        out_specs=(P("gr", "sp", "tp", None), P("gr", "sp", "tp"), P("gr", "sp", None)),
        check_vma=False,
    )
```

```python
import functools

import jax
import jax.numpy as jnp
from jax import lax
from jax.experimental import pallas as pl
from jax.experimental.pallas import tpu as pltpu
from jax.sharding import PartitionSpec as P

MESH = pl.DeviceIdType.MESH
LANES = 128


def partner(step, me, n, turned=0):
    turn, flip = step // 2, lax.rem(step + turned, 2)
    flip = jnp.where(turn == n // 2 - 1, 1 - lax.rem(step, 2), flip)
    half = n // 4
    at = me // 2
    far = at >= half
    w = jnp.where(far, 2 * half - 1 - at, at)
    goal = jnp.where(turn < half, 2 * half - 1 - turn, lax.rem(w + 1 + turn, half))
    goal = jnp.where(far, 2 * half - 1 - goal, goal)
    return goal * 2 + lax.rem(me + flip, 2)


def exchange_kernel(
    n, per_owner, tile, head,
    tokens, key_weight, value_weight, gates, query,
    kv, outgoing, gate_out, read,
    rows, weights, gate_own, gate_send, gate_in, query_own, query_in, part_send, part_in, mine, theirs,
    row_sem, weight_sem, small_sem, send_sem, recv_sem,
    gate_sent, gate_recv, query_sent, query_recv, part_sent, part_recv, pair_sem,
):
    me = lax.axis_index("sp")
    core = lax.axis_index("tp")
    count = rows.shape[0]
    tiles = count // tile
    early = max(tiles - 1, 1)
    columns = weights.shape[3]
    group_heads = columns // head
    owners = group_heads // per_owner
    groups = n // owners

    def group_of(step):
        if owners == 1:
            return partner(step, me, n, core)
        return lax.rem(me // owners + 1 + step, groups)

    def load_rows(t):
        span = pl.ds(t * tile, tile)
        return pltpu.make_async_copy(tokens.at[span, :], rows.at[span, :], row_sem.at[t])

    def load_weight(step, which):
        at = pl.ds(pl.multiple_of(group_of(step) * columns, columns), columns)
        source = (key_weight, value_weight)[which]
        return pltpu.make_async_copy(
            source.at[:, at], weights.at[step, which], weight_sem.at[step, which]
        )

    load_query = pltpu.make_async_copy(query, query_own, small_sem.at[0])
    load_gates = pltpu.make_async_copy(gates, gate_own, small_sem.at[1])
    load_query.start()
    load_rows(0).start()
    load_weight(0, 0).start()
    load_weight(0, 1).start()
    load_gates.start()
    for t in range(1, tiles):
        load_rows(t).start()

    barrier = pltpu.get_barrier_semaphore()

    @pl.loop(1, n)
    def _(k):
        pl.semaphore_signal(
            barrier, inc=1, device_id={"sp": lax.rem(me + k, n)}, device_id_type=MESH
        )

    pl.semaphore_signal(barrier, inc=1, device_id={"tp": 1 - core}, device_id_type=MESH)

    def query_copy(owner):
        return pltpu.make_async_remote_copy(
            src_ref=query_in.at[me], dst_ref=query_in.at[me],
            send_sem=query_sent.at[owner], recv_sem=query_recv.at[me],
            device_id={"sp": owner}, device_id_type=MESH,
        )

    def gate_copy(owner):
        return pltpu.make_async_remote_copy(
            src_ref=gate_send.at[owner], dst_ref=gate_in.at[me],
            send_sem=gate_sent.at[owner], recv_sem=gate_recv.at[me],
            device_id={"sp": owner}, device_id_type=MESH,
        )

    def part_copy(owner):
        return pltpu.make_async_remote_copy(
            src_ref=part_send.at[owner], dst_ref=part_in.at[me],
            send_sem=part_sent.at[owner], recv_sem=part_recv.at[me],
            device_id={"sp": owner}, device_id_type=MESH,
        )

    def block_copy(owner, t):
        return pltpu.make_async_remote_copy(
            src_ref=outgoing.at[owner, :, pl.ds(t * tile, tile), :],
            dst_ref=kv.at[:, pl.ds(pl.multiple_of(me * count + t * tile, tile), tile), :],
            send_sem=send_sem.at[owner, t], recv_sem=recv_sem.at[me, t],
            device_id={"sp": owner}, device_id_type=MESH,
        )

    def block_own(t):
        return pltpu.make_async_copy(
            outgoing.at[me, :, pl.ds(t * tile, tile), :],
            kv.at[:, pl.ds(pl.multiple_of(me * count + t * tile, tile), tile), :],
            recv_sem.at[me, t],
        )

    def send_block(owner, t):
        @pl.when(owner != me)
        def _():
            block_copy(owner, t).start()

        @pl.when(owner == me)
        def _():
            block_own(t).start()

    def own_gates(owner, span):
        return jnp.concatenate([gate_own[owner, h, :, span] for h in range(per_owner)], axis=0)

    low = lax.broadcasted_iota(jnp.int32, (tile, LANES), 1) < head

    def open_links():
        pl.semaphore_wait(barrier, n)

    def send_queries():
        load_gates.wait()
        load_query.wait()
        query_in[me] = jnp.concatenate(
            [query_own[...].astype(jnp.float32), jnp.zeros((per_owner, LANES - head), jnp.float32)], axis=1
        ) * (head ** -0.5)

        @pl.loop(0, n - 1)
        def _(k):
            query_copy(partner(k, me, n)).start()

    def send_gates():
        @pl.loop(0, n - 1)
        def _(k):
            owner = partner(k, me, n)
            gate_send[owner] = own_gates(owner, slice(None)).astype(jnp.bfloat16)
            gate_copy(owner).start()

        gate_in[me] = own_gates(me, slice(None)).astype(jnp.bfloat16)

    head_row = lax.broadcasted_iota(jnp.int32, (per_owner, LANES), 0)
    tile_row = lax.broadcasted_iota(jnp.int32, (per_owner, tile), 0)
    lane = lax.broadcasted_iota(jnp.int32, (per_owner, LANES), 1)

    def read_own(owner):
        @pl.when(owner != me)
        def _():
            pltpu.make_async_copy(query_in.at[owner], query_in.at[owner], query_recv.at[owner]).wait()

        asked = query_in[owner]
        queries = [
            jnp.where(head_row == h, asked, 0.0).astype(jnp.bfloat16) for h in range(per_owner)
        ]
        top = jnp.full((per_owner, 1), -1e30, jnp.float32)
        total = jnp.zeros((per_owner, 1), jnp.float32)
        weighted = jnp.zeros((per_owner, LANES), jnp.float32)
        for t in range(tiles):
            span = pl.ds(t * tile, tile)
            blocks = [outgoing[owner, h, span, :] for h in range(per_owner)]
            scores = None
            for h in range(per_owner):
                term = lax.dot_general(
                    queries[h], blocks[h], (((1,), (1,)), ((), ())), preferred_element_type=jnp.float32
                )
                scores = term if scores is None else scores + term
            scores = scores - own_gates(owner, span)
            new_top = jnp.maximum(top, jnp.max(scores, axis=1, keepdims=True))
            scale = jnp.exp(top - new_top)
            probs = jnp.exp(scores - new_top)
            total = total * scale + jnp.sum(probs, axis=1, keepdims=True)
            weighted = weighted * scale
            for h in range(per_owner):
                picked = jnp.where(tile_row == h, probs, 0.0).astype(jnp.bfloat16)
                weighted = weighted + jnp.dot(picked, blocks[h], preferred_element_type=jnp.float32)
            top = new_top
        packed = jnp.where(lane < head // 2, top, jnp.where(lane < head, total, weighted))
        part_send[owner] = packed

        @pl.when(owner != me)
        def _():
            part_copy(owner).start()

    def project(step, first):
        group = group_of(step)

        if first:
            for ahead in range(1, min(3, groups)):
                load_weight(ahead, 0).start()
                load_weight(ahead, 1).start()
        else:
            @pl.when(step + 2 < groups)
            def _():
                load_weight(step + 2, 0).start()
                load_weight(step + 2, 1).start()

        load_weight(step, 0).wait()
        load_weight(step, 1).wait()
        for t in range(tiles):
            if first:
                load_rows(t).wait()
            left = rows[pl.ds(t * tile, tile), :]
            keys = jnp.dot(left, weights[step, 0], preferred_element_type=jnp.float32)
            values = jnp.dot(left, weights[step, 1], preferred_element_type=jnp.float32)
            for pair in range(columns // LANES):
                span = slice(pair * LANES, (pair + 1) * LANES)
                k, v = keys[:, span], values[:, span]
                joined = (
                    jnp.where(low, k, pltpu.roll(v, head, 1)),
                    jnp.where(low, pltpu.roll(k, head, 1), v),
                )
                for half in range(2):
                    local = pair * 2 + half
                    owner = group * owners + local // per_owner
                    outgoing[owner, local % per_owner, pl.ds(t * tile, tile), :] = joined[
                        half
                    ].astype(jnp.bfloat16)
            if first and t == 0:
                open_links()
            if t < early:
                for j in range(owners):
                    send_block(group * owners + j, t)
            if first and t == 0:
                send_queries()
        for j in range(owners):
            read_own(group * owners + j)

    project(0, True)
    send_gates()

    def later(step, carry):
        project(step, False)
        return carry

    lax.fori_loop(1, groups, later, 0)

    if early < tiles:
        @pl.when(core == 0)
        def _():
            @pl.loop(0, n)
            def _(k):
                for t in range(early, tiles):
                    send_block(partner(k, me, n), t)

    @pl.loop(0, n - 1)
    def _(k):
        source = partner(k, me, n)
        gate_copy(source).wait_send()
        query_copy(source).wait_send()
        pltpu.make_async_copy(gate_in.at[source], gate_in.at[source], gate_recv.at[source]).wait()

    for source in range(n):
        gate_out[:, source * count:(source + 1) * count] = gate_in[source].astype(jnp.float32)

    def merge(one, two):
        top_one, top_two = one[:, :1], two[:, :1]
        joint = jnp.maximum(top_one, top_two)
        both = one * jnp.exp(top_one - joint) + two * jnp.exp(top_two - joint)
        return jnp.where(lane < head // 2, joint, both)

    def gather(k, carry):
        source = partner(n - 2 - k, me, n)
        part_copy(source).wait_send()
        pltpu.make_async_copy(part_in.at[source], part_in.at[source], part_recv.at[source]).wait()
        return merge(carry, part_in[source])

    packed = lax.fori_loop(0, n - 1, gather, part_send[me])
    mine[...] = packed
    swap = pltpu.make_async_remote_copy(
        src_ref=mine, dst_ref=theirs, send_sem=pair_sem.at[0], recv_sem=pair_sem.at[1],
        device_id={"tp": 1 - core}, device_id_type=MESH,
    )
    swap.start()
    swap.wait()
    other = theirs[...]
    joint = merge(jnp.where(core == 0, packed, other), jnp.where(core == 0, other, packed))
    at = head // 2
    answer = joint / joint[:, at:at + 1]
    read[...] = pltpu.roll(answer, head, 1)[:, :head].astype(jnp.bfloat16)

    def settle(t):
        block_own(t).wait()

        @pl.loop(0, n - 1)
        def _(k):
            source = partner(n - 2 - k, me, n)
            block_copy(source, t).wait_send()
            pltpu.make_async_copy(
                kv.at[:, pl.ds(t * tile, tile), :], kv.at[:, pl.ds(t * tile, tile), :], recv_sem.at[source, t]
            ).wait()

    for t in range(early):
        settle(t)
    if early < tiles:
        @pl.when(core == 0)
        def _():
            for t in range(early, tiles):
                settle(t)


def rest_kernel(
    n, first_row,
    outgoing, after,
    late,
    send_sem, recv_sem,
):
    me = lax.axis_index("sp")
    size = outgoing.shape[2] - first_row
    held = pl.ds(first_row, size)

    def rows_of(source):
        return pl.ds(pl.multiple_of(source * size, size), size)

    def block_copy(owner):
        return pltpu.make_async_remote_copy(
            src_ref=outgoing.at[owner, :, held, :], dst_ref=late.at[:, rows_of(me), :],
            send_sem=send_sem.at[owner], recv_sem=recv_sem.at[me],
            device_id={"sp": owner}, device_id_type=MESH,
        )

    @pl.when(lax.axis_index("tp") == 1)
    def _():
        barrier = pltpu.get_barrier_semaphore()

        @pl.loop(1, n)
        def _(k):
            pl.semaphore_signal(
                barrier, inc=1, device_id={"sp": lax.rem(me + k, n)}, device_id_type=MESH
            )

        pl.semaphore_wait(barrier, n - 1)

        @pl.loop(0, n - 1)
        def _(k):
            block_copy(partner(k, me, n)).start()

        late[:, rows_of(me), :] = outgoing[me, :, held, :]

        @pl.loop(0, n - 1)
        def _(k):
            source = partner(n - 2 - k, me, n)
            block_copy(source).wait_send()
            pltpu.make_async_copy(
                outgoing.at[0, :, held, :], late.at[:, rows_of(source), :], recv_sem.at[source]
            ).wait()


def finish_kernel(n, first_row, kv, gates, answer, kv_out, gate_out, read, sem):
    count = kv.shape[1] // n

    def part(source, start, size, at):
        span = pl.ds(source * count + start, size)
        return pltpu.make_async_copy(kv.at[:, span, :], kv_out.at[:, span, :], sem.at[at])

    small = [
        pltpu.make_async_copy(gates, gate_out, sem.at[2 * n]),
        pltpu.make_async_copy(answer, read, sem.at[2 * n + 1]),
    ]
    early = [part(source, 0, first_row, source) for source in range(n)]
    for copy in early + small:
        copy.start()
    if first_row < count:
        @pl.when(lax.axis_index("tp") == 0)
        def _():
            late = [part(source, first_row, count - first_row, n + source) for source in range(n)]
            for copy in late:
                copy.start()
            for copy in late:
                copy.wait()
    for copy in early + small:
        copy.wait()


def last_kernel(n, first_row, late, kv, kv_out, sem):
    count = kv_out.shape[1] // n
    size = count - first_row

    @pl.when(lax.axis_index("tp") == 1)
    def _():
        copies = [
            pltpu.make_async_copy(
                late.at[:, pl.ds(source * size, size), :],
                kv_out.at[:, pl.ds(source * count + first_row, size), :],
                sem.at[source],
            )
            for source in range(n)
        ]
        for copy in copies:
            copy.start()
        for copy in copies:
            copy.wait()


def on_device(n, tokens, key_weight, value_weight, cum_gate, query):
    _, _, count, width = tokens.shape
    heads = cum_gate.shape[1]
    per_owner, head = query.shape[1], query.shape[2]
    tile = 256 if count % 256 == 0 else count
    columns = max(per_owner * head, LANES)
    groups = heads * head // columns
    tiles = count // tile
    any_space = pl.BlockSpec(memory_space=pl.ANY)
    outside = pl.BlockSpec(memory_space=pltpu.HBM)
    vmem = pl.BlockSpec(memory_space=pltpu.VMEM)
    kv, outgoing, gates, answer = pl.pallas_call(
        functools.partial(exchange_kernel, n, per_owner, tile, head),
        name="exchange",
        out_shape=(
            pltpu.VMEM((per_owner, n * count, 2 * head), jnp.bfloat16),
            pltpu.VMEM((n, per_owner, count, 2 * head), jnp.bfloat16),
            pltpu.VMEM((per_owner, n * count), jnp.float32),
            pltpu.VMEM((per_owner, head), jnp.bfloat16),
        ),
        in_specs=[outside] * 5,
        out_specs=(vmem, vmem, vmem, vmem),
        scratch_shapes=[
            pltpu.VMEM((count, width), jnp.bfloat16),
            pltpu.VMEM((groups, 2, width, columns), jnp.bfloat16),
            pltpu.VMEM((n, per_owner, 1, count), jnp.float32),
            pltpu.VMEM((n, per_owner, count), jnp.bfloat16),
            pltpu.VMEM((n, per_owner, count), jnp.bfloat16),
            pltpu.VMEM((per_owner, head), jnp.bfloat16),
            pltpu.VMEM((n, per_owner, LANES), jnp.float32),
            pltpu.VMEM((n, per_owner, LANES), jnp.float32),
            pltpu.VMEM((n, per_owner, LANES), jnp.float32),
            pltpu.VMEM((per_owner, LANES), jnp.float32),
            pltpu.VMEM((per_owner, LANES), jnp.float32),
            pltpu.SemaphoreType.DMA((tiles,)),
            pltpu.SemaphoreType.DMA((groups, 2)),
            pltpu.SemaphoreType.DMA((2,)),
            pltpu.SemaphoreType.DMA((n, tiles)),
            pltpu.SemaphoreType.DMA((n, tiles)),
            pltpu.SemaphoreType.DMA((n,)),
            pltpu.SemaphoreType.DMA((n,)),
            pltpu.SemaphoreType.DMA((n,)),
            pltpu.SemaphoreType.DMA((n,)),
            pltpu.SemaphoreType.DMA((n,)),
            pltpu.SemaphoreType.DMA((n,)),
            pltpu.SemaphoreType.DMA((2,)),
        ],
        compiler_params=pltpu.CompilerParams(
            collective_id=0, has_side_effects=True, vmem_limit_bytes=48 * 1024 * 1024
        ),
    )(
        tokens.reshape(count, width),
        key_weight,
        value_weight,
        cum_gate.reshape(n, per_owner, 1, count),
        query.reshape(per_owner, head),
    )
    first_row = max(tiles - 1, 1) * tile
    whole = jax.ShapeDtypeStruct((per_owner, n * count, 2 * head), jnp.bfloat16)
    kv_out, gate_out, read = pl.pallas_call(
        functools.partial(finish_kernel, n, first_row),
        name="finish",
        out_shape=(
            whole,
            jax.ShapeDtypeStruct((per_owner, n * count), jnp.float32),
            jax.ShapeDtypeStruct((per_owner, head), jnp.bfloat16),
        ),
        in_specs=[vmem, vmem, vmem],
        out_specs=(any_space, any_space, any_space),
        scratch_shapes=[pltpu.SemaphoreType.DMA((2 * n + 2,))],
        compiler_params=pltpu.CompilerParams(vmem_limit_bytes=16 * 1024 * 1024),
    )(kv, gates, answer)
    if first_row < count:
        late = pl.pallas_call(
            functools.partial(rest_kernel, n, first_row),
            name="rest",
            out_shape=pltpu.VMEM((per_owner, n * (count - first_row), 2 * head), jnp.bfloat16),
            in_specs=[vmem, outside],
            out_specs=vmem,
            scratch_shapes=[pltpu.SemaphoreType.DMA((n,)), pltpu.SemaphoreType.DMA((n,))],
            compiler_params=pltpu.CompilerParams(
                collective_id=1, has_side_effects=True, vmem_limit_bytes=48 * 1024 * 1024
            ),
        )(outgoing, read)
        kv_out = pl.pallas_call(
            functools.partial(last_kernel, n, first_row),
            name="last",
            out_shape=whole,
            in_specs=[vmem, any_space],
            out_specs=any_space,
            input_output_aliases={1: 0},
            scratch_shapes=[pltpu.SemaphoreType.DMA((n,))],
            compiler_params=pltpu.CompilerParams(vmem_limit_bytes=16 * 1024 * 1024),
        )(late, kv_out)
    return kv_out[None], gate_out[None], read[None]


def solution(mesh):
    placed = (P("gr", "tp", "sp", None), P(), P(), P("gr", None, "tp", "sp"), P("gr", "sp", None))
    return jax.shard_map(
        functools.partial(on_device, mesh.shape["sp"]),
        mesh=mesh,
        in_specs=placed,
        out_specs=(P("gr", "sp", "tp", None), P("gr", "sp", "tp"), P("gr", "sp", None)),
        check_vma=False,
    )
```

```python
import functools

import jax
import jax.numpy as jnp
from jax import lax
from jax.experimental import pallas as pl
from jax.experimental.pallas import tpu as pltpu
from jax.sharding import PartitionSpec as P

MESH = pl.DeviceIdType.MESH
LANES = 128


def partner(step, me, n, turned=0):
    turn, flip = step // 2, lax.rem(step + turned, 2)
    flip = jnp.where(turn == n // 2 - 1, 1 - lax.rem(step, 2), flip)
    half = n // 4
    at = me // 2
    far = at >= half
    w = jnp.where(far, 2 * half - 1 - at, at)
    goal = jnp.where(turn < half, 2 * half - 1 - turn, lax.rem(w + 1 + turn, half))
    goal = jnp.where(far, 2 * half - 1 - goal, goal)
    return goal * 2 + lax.rem(me + flip, 2)


def exchange_kernel(
    n, per_owner, tile, head,
    tokens, key_weight, value_weight, gates, query,
    kv, outgoing, gate_out, read,
    rows, weights, gate_own, gate_send, gate_in, query_own, query_in, part_send, part_in, mine, theirs,
    row_sem, weight_sem, small_sem, send_sem, recv_sem,
    gate_sent, gate_recv, query_sent, query_recv, part_sent, part_recv, pair_sem,
):
    me = lax.axis_index("sp")
    core = lax.axis_index("tp")
    count = rows.shape[0]
    tiles = count // tile
    early = max(tiles - 1, 1)
    columns = weights.shape[3]
    group_heads = columns // head
    owners = group_heads // per_owner
    groups = n // owners

    def group_of(step):
        if owners == 1:
            return partner(step, me, n, core)
        return lax.rem(me // owners + 1 + step, groups)

    def load_rows(t):
        span = pl.ds(t * tile, tile)
        return pltpu.make_async_copy(tokens.at[span, :], rows.at[span, :], row_sem.at[t])

    def load_weight(step, which):
        at = pl.ds(pl.multiple_of(group_of(step) * columns, columns), columns)
        source = (key_weight, value_weight)[which]
        return pltpu.make_async_copy(
            source.at[:, at], weights.at[step, which], weight_sem.at[step, which]
        )

    load_query = pltpu.make_async_copy(query, query_own, small_sem.at[0])
    load_gates = pltpu.make_async_copy(gates, gate_own, small_sem.at[1])
    load_query.start()
    load_rows(0).start()
    load_weight(0, 0).start()
    load_weight(0, 1).start()
    load_gates.start()
    for t in range(1, tiles):
        load_rows(t).start()

    barrier = pltpu.get_barrier_semaphore()

    @pl.loop(1, n)
    def _(k):
        pl.semaphore_signal(
            barrier, inc=1, device_id={"sp": lax.rem(me + k, n)}, device_id_type=MESH
        )

    pl.semaphore_signal(barrier, inc=1, device_id={"tp": 1 - core}, device_id_type=MESH)

    def query_copy(owner):
        return pltpu.make_async_remote_copy(
            src_ref=query_in.at[me], dst_ref=query_in.at[me],
            send_sem=query_sent.at[owner], recv_sem=query_recv.at[me],
            device_id={"sp": owner}, device_id_type=MESH,
        )

    def gate_copy(owner):
        return pltpu.make_async_remote_copy(
            src_ref=gate_send.at[owner], dst_ref=gate_in.at[me],
            send_sem=gate_sent.at[owner], recv_sem=gate_recv.at[me],
            device_id={"sp": owner}, device_id_type=MESH,
        )

    def part_copy(owner):
        return pltpu.make_async_remote_copy(
            src_ref=part_send.at[owner], dst_ref=part_in.at[me],
            send_sem=part_sent.at[owner], recv_sem=part_recv.at[me],
            device_id={"sp": owner}, device_id_type=MESH,
        )

    def block_copy(owner, t):
        return pltpu.make_async_remote_copy(
            src_ref=outgoing.at[owner, :, pl.ds(t * tile, tile), :],
            dst_ref=kv.at[:, pl.ds(pl.multiple_of(me * count + t * tile, tile), tile), :],
            send_sem=send_sem.at[owner, t], recv_sem=recv_sem.at[me, t],
            device_id={"sp": owner}, device_id_type=MESH,
        )

    def block_own(t):
        return pltpu.make_async_copy(
            outgoing.at[me, :, pl.ds(t * tile, tile), :],
            kv.at[:, pl.ds(pl.multiple_of(me * count + t * tile, tile), tile), :],
            recv_sem.at[me, t],
        )

    def send_block(owner, t):
        @pl.when(owner != me)
        def _():
            block_copy(owner, t).start()

        @pl.when(owner == me)
        def _():
            block_own(t).start()

    def own_gates(owner, span):
        return jnp.concatenate([gate_own[owner, h, :, span] for h in range(per_owner)], axis=0)

    low = lax.broadcasted_iota(jnp.int32, (tile, LANES), 1) < head

    def open_links():
        pl.semaphore_wait(barrier, n)

    def send_queries():
        load_gates.wait()
        load_query.wait()
        query_in[me] = jnp.concatenate(
            [query_own[...].astype(jnp.float32), jnp.zeros((per_owner, LANES - head), jnp.float32)], axis=1
        ) * (head ** -0.5)

        @pl.loop(0, n - 1)
        def _(k):
            query_copy(partner(k, me, n)).start()

    def send_gates():
        @pl.loop(0, n - 1)
        def _(k):
            owner = partner(k, me, n)
            gate_send[owner] = own_gates(owner, slice(None)).astype(jnp.bfloat16)
            gate_copy(owner).start()

        gate_in[me] = own_gates(me, slice(None)).astype(jnp.bfloat16)

    head_row = lax.broadcasted_iota(jnp.int32, (per_owner, LANES), 0)
    tile_row = lax.broadcasted_iota(jnp.int32, (per_owner, tile), 0)
    lane = lax.broadcasted_iota(jnp.int32, (per_owner, LANES), 1)

    def read_own(owner):
        @pl.when(owner != me)
        def _():
            pltpu.make_async_copy(query_in.at[owner], query_in.at[owner], query_recv.at[owner]).wait()

        asked = query_in[owner]
        queries = [
            jnp.where(head_row == h, asked, 0.0).astype(jnp.bfloat16) for h in range(per_owner)
        ]
        top = jnp.full((per_owner, 1), -1e30, jnp.float32)
        total = jnp.zeros((per_owner, 1), jnp.float32)
        weighted = jnp.zeros((per_owner, LANES), jnp.float32)
        for t in range(tiles):
            span = pl.ds(t * tile, tile)
            blocks = [outgoing[owner, h, span, :] for h in range(per_owner)]
            scores = None
            for h in range(per_owner):
                term = lax.dot_general(
                    queries[h], blocks[h], (((1,), (1,)), ((), ())), preferred_element_type=jnp.float32
                )
                scores = term if scores is None else scores + term
            scores = scores - own_gates(owner, span)
            new_top = jnp.maximum(top, jnp.max(scores, axis=1, keepdims=True))
            scale = jnp.exp(top - new_top)
            probs = jnp.exp(scores - new_top)
            total = total * scale + jnp.sum(probs, axis=1, keepdims=True)
            weighted = weighted * scale
            for h in range(per_owner):
                picked = jnp.where(tile_row == h, probs, 0.0).astype(jnp.bfloat16)
                weighted = weighted + jnp.dot(picked, blocks[h], preferred_element_type=jnp.float32)
            top = new_top
        packed = jnp.where(lane < head // 2, top, jnp.where(lane < head, total, weighted))
        part_send[owner] = packed

        @pl.when(owner != me)
        def _():
            part_copy(owner).start()

    def project(step, first):
        group = group_of(step)

        if first:
            for ahead in range(1, min(3, groups)):
                load_weight(ahead, 0).start()
                load_weight(ahead, 1).start()
        else:
            @pl.when(step + 2 < groups)
            def _():
                load_weight(step + 2, 0).start()
                load_weight(step + 2, 1).start()

        load_weight(step, 0).wait()
        load_weight(step, 1).wait()
        for t in range(tiles):
            if first:
                load_rows(t).wait()
            left = rows[pl.ds(t * tile, tile), :]
            keys = jnp.dot(left, weights[step, 0], preferred_element_type=jnp.float32)
            values = jnp.dot(left, weights[step, 1], preferred_element_type=jnp.float32)
            for pair in range(columns // LANES):
                span = slice(pair * LANES, (pair + 1) * LANES)
                k, v = keys[:, span], values[:, span]
                joined = (
                    jnp.where(low, k, pltpu.roll(v, head, 1)),
                    jnp.where(low, pltpu.roll(k, head, 1), v),
                )
                for half in range(2):
                    local = pair * 2 + half
                    owner = group * owners + local // per_owner
                    outgoing[owner, local % per_owner, pl.ds(t * tile, tile), :] = joined[
                        half
                    ].astype(jnp.bfloat16)
            if first and t == 0:
                open_links()
            if t < early:
                for j in range(owners):
                    send_block(group * owners + j, t)
            if first and t == 0:
                send_queries()
        for j in range(owners):
            read_own(group * owners + j)

    project(0, True)
    send_gates()

    def later(step, carry):
        project(step, False)
        return carry

    lax.fori_loop(1, groups, later, 0)

    if early < tiles:
        @pl.when(core == 0)
        def _():
            @pl.loop(0, n)
            def _(k):
                for t in range(early, tiles):
                    send_block(partner(k, me, n), t)

    @pl.loop(0, n - 1)
    def _(k):
        source = partner(k, me, n)
        gate_copy(source).wait_send()
        query_copy(source).wait_send()
        pltpu.make_async_copy(gate_in.at[source], gate_in.at[source], gate_recv.at[source]).wait()

    for source in range(n):
        gate_out[:, source * count:(source + 1) * count] = gate_in[source].astype(jnp.float32)

    def merge(one, two):
        top_one, top_two = one[:, :1], two[:, :1]
        joint = jnp.maximum(top_one, top_two)
        both = one * jnp.exp(top_one - joint) + two * jnp.exp(top_two - joint)
        return jnp.where(lane < head // 2, joint, both)

    def gather(k, carry):
        source = partner(n - 2 - k, me, n)
        part_copy(source).wait_send()
        pltpu.make_async_copy(part_in.at[source], part_in.at[source], part_recv.at[source]).wait()
        return merge(carry, part_in[source])

    packed = lax.fori_loop(0, n - 1, gather, part_send[me])
    mine[...] = packed
    swap = pltpu.make_async_remote_copy(
        src_ref=mine, dst_ref=theirs, send_sem=pair_sem.at[0], recv_sem=pair_sem.at[1],
        device_id={"tp": 1 - core}, device_id_type=MESH,
    )
    swap.start()
    swap.wait()
    other = theirs[...]
    joint = merge(jnp.where(core == 0, packed, other), jnp.where(core == 0, other, packed))
    at = head // 2
    answer = joint / joint[:, at:at + 1]
    read[...] = pltpu.roll(answer, head, 1)[:, :head].astype(jnp.bfloat16)

    def settle(t):
        block_own(t).wait()

        @pl.loop(0, n - 1)
        def _(k):
            source = partner(n - 2 - k, me, n)
            block_copy(source, t).wait_send()
            pltpu.make_async_copy(
                kv.at[:, pl.ds(t * tile, tile), :], kv.at[:, pl.ds(t * tile, tile), :], recv_sem.at[source, t]
            ).wait()

    for t in range(early):
        settle(t)
    if early < tiles:
        @pl.when(core == 0)
        def _():
            for t in range(early, tiles):
                settle(t)


def rest_kernel(
    n, first_row,
    outgoing, after,
    late,
    send_sem, recv_sem,
):
    me = lax.axis_index("sp")
    size = outgoing.shape[2] - first_row
    held = pl.ds(first_row, size)

    def rows_of(source):
        return pl.ds(pl.multiple_of(source * size, size), size)

    def block_copy(owner):
        return pltpu.make_async_remote_copy(
            src_ref=outgoing.at[owner, :, held, :], dst_ref=late.at[:, rows_of(me), :],
            send_sem=send_sem.at[owner], recv_sem=recv_sem.at[me],
            device_id={"sp": owner}, device_id_type=MESH,
        )

    @pl.when(lax.axis_index("tp") == 1)
    def _():
        barrier = pltpu.get_barrier_semaphore()

        @pl.loop(1, n)
        def _(k):
            pl.semaphore_signal(
                barrier, inc=1, device_id={"sp": lax.rem(me + k, n)}, device_id_type=MESH
            )

        pl.semaphore_wait(barrier, n - 1)

        @pl.loop(0, n - 1)
        def _(k):
            block_copy(partner(k, me, n)).start()

        late[:, rows_of(me), :] = outgoing[me, :, held, :]

        @pl.loop(0, n - 1)
        def _(k):
            source = partner(n - 2 - k, me, n)
            block_copy(source).wait_send()
            pltpu.make_async_copy(
                outgoing.at[0, :, held, :], late.at[:, rows_of(source), :], recv_sem.at[source]
            ).wait()


def finish_kernel(n, first_row, kv, gates, answer, kv_out, gate_out, read, after, sem):
    count = kv.shape[1] // n

    def part(source, start, size, at):
        span = pl.ds(source * count + start, size)
        return pltpu.make_async_copy(kv.at[:, span, :], kv_out.at[:, span, :], sem.at[at])

    small = [
        pltpu.make_async_copy(gates, gate_out, sem.at[2 * n]),
        pltpu.make_async_copy(answer, read, sem.at[2 * n + 1]),
    ]
    early = [part(source, 0, first_row, source) for source in range(n)]
    for copy in early + small:
        copy.start()
    after[...] = jnp.zeros_like(after)
    if first_row < count:
        @pl.when(lax.axis_index("tp") == 0)
        def _():
            late = [part(source, first_row, count - first_row, n + source) for source in range(n)]
            for copy in late:
                copy.start()
            for copy in late:
                copy.wait()
    for copy in early + small:
        copy.wait()


def last_kernel(n, first_row, late, kv, kv_out, sem):
    count = kv_out.shape[1] // n
    size = count - first_row

    @pl.when(lax.axis_index("tp") == 1)
    def _():
        copies = [
            pltpu.make_async_copy(
                late.at[:, pl.ds(source * size, size), :],
                kv_out.at[:, pl.ds(source * count + first_row, size), :],
                sem.at[source],
            )
            for source in range(n)
        ]
        for copy in copies:
            copy.start()
        for copy in copies:
            copy.wait()


def on_device(n, tokens, key_weight, value_weight, cum_gate, query):
    _, _, count, width = tokens.shape
    heads = cum_gate.shape[1]
    per_owner, head = query.shape[1], query.shape[2]
    tile = 256 if count % 256 == 0 else count
    columns = max(per_owner * head, LANES)
    groups = heads * head // columns
    tiles = count // tile
    any_space = pl.BlockSpec(memory_space=pl.ANY)
    outside = pl.BlockSpec(memory_space=pltpu.HBM)
    vmem = pl.BlockSpec(memory_space=pltpu.VMEM)
    kv, outgoing, gates, answer = pl.pallas_call(
        functools.partial(exchange_kernel, n, per_owner, tile, head),
        name="exchange",
        out_shape=(
            pltpu.VMEM((per_owner, n * count, 2 * head), jnp.bfloat16),
            pltpu.VMEM((n, per_owner, count, 2 * head), jnp.bfloat16),
            pltpu.VMEM((per_owner, n * count), jnp.float32),
            pltpu.VMEM((per_owner, head), jnp.bfloat16),
        ),
        in_specs=[outside] * 5,
        out_specs=(vmem, vmem, vmem, vmem),
        scratch_shapes=[
            pltpu.VMEM((count, width), jnp.bfloat16),
            pltpu.VMEM((groups, 2, width, columns), jnp.bfloat16),
            pltpu.VMEM((n, per_owner, 1, count), jnp.float32),
            pltpu.VMEM((n, per_owner, count), jnp.bfloat16),
            pltpu.VMEM((n, per_owner, count), jnp.bfloat16),
            pltpu.VMEM((per_owner, head), jnp.bfloat16),
            pltpu.VMEM((n, per_owner, LANES), jnp.float32),
            pltpu.VMEM((n, per_owner, LANES), jnp.float32),
            pltpu.VMEM((n, per_owner, LANES), jnp.float32),
            pltpu.VMEM((per_owner, LANES), jnp.float32),
            pltpu.VMEM((per_owner, LANES), jnp.float32),
            pltpu.SemaphoreType.DMA((tiles,)),
            pltpu.SemaphoreType.DMA((groups, 2)),
            pltpu.SemaphoreType.DMA((2,)),
            pltpu.SemaphoreType.DMA((n, tiles)),
            pltpu.SemaphoreType.DMA((n, tiles)),
            pltpu.SemaphoreType.DMA((n,)),
            pltpu.SemaphoreType.DMA((n,)),
            pltpu.SemaphoreType.DMA((n,)),
            pltpu.SemaphoreType.DMA((n,)),
            pltpu.SemaphoreType.DMA((n,)),
            pltpu.SemaphoreType.DMA((n,)),
            pltpu.SemaphoreType.DMA((2,)),
        ],
        compiler_params=pltpu.CompilerParams(
            collective_id=0, has_side_effects=True, vmem_limit_bytes=48 * 1024 * 1024
        ),
    )(
        tokens.reshape(count, width),
        key_weight,
        value_weight,
        cum_gate.reshape(n, per_owner, 1, count),
        query.reshape(per_owner, head),
    )
    first_row = max(tiles - 1, 1) * tile
    whole = jax.ShapeDtypeStruct((per_owner, n * count, 2 * head), jnp.bfloat16)
    kv_out, gate_out, read, after = pl.pallas_call(
        functools.partial(finish_kernel, n, first_row),
        name="finish",
        out_shape=(
            whole,
            jax.ShapeDtypeStruct((per_owner, n * count), jnp.float32),
            jax.ShapeDtypeStruct((per_owner, head), jnp.bfloat16),
            pltpu.VMEM((8, LANES), jnp.float32),
        ),
        in_specs=[vmem, vmem, vmem],
        out_specs=(any_space, any_space, any_space, vmem),
        scratch_shapes=[pltpu.SemaphoreType.DMA((2 * n + 2,))],
        compiler_params=pltpu.CompilerParams(vmem_limit_bytes=16 * 1024 * 1024),
    )(kv, gates, answer)
    if first_row < count:
        late = pl.pallas_call(
            functools.partial(rest_kernel, n, first_row),
            name="rest",
            out_shape=pltpu.VMEM((per_owner, n * (count - first_row), 2 * head), jnp.bfloat16),
            in_specs=[vmem, vmem],
            out_specs=vmem,
            scratch_shapes=[pltpu.SemaphoreType.DMA((n,)), pltpu.SemaphoreType.DMA((n,))],
            compiler_params=pltpu.CompilerParams(
                collective_id=1, has_side_effects=True, vmem_limit_bytes=16 * 1024 * 1024
            ),
        )(outgoing, after)
        kv_out = pl.pallas_call(
            functools.partial(last_kernel, n, first_row),
            name="last",
            out_shape=whole,
            in_specs=[vmem, any_space],
            out_specs=any_space,
            input_output_aliases={1: 0},
            scratch_shapes=[pltpu.SemaphoreType.DMA((n,))],
            compiler_params=pltpu.CompilerParams(vmem_limit_bytes=16 * 1024 * 1024),
        )(late, kv_out)
    return kv_out[None], gate_out[None], read[None]


def solution(mesh):
    placed = (P("gr", "tp", "sp", None), P(), P(), P("gr", None, "tp", "sp"), P("gr", "sp", None))
    return jax.shard_map(
        functools.partial(on_device, mesh.shape["sp"]),
        mesh=mesh,
        in_specs=placed,
        out_specs=(P("gr", "sp", "tp", None), P("gr", "sp", "tp"), P("gr", "sp", None)),
        check_vma=False,
    )
```

```python
import functools

import jax
import jax.numpy as jnp
from jax import lax
from jax.experimental import pallas as pl
from jax.experimental.pallas import tpu as pltpu
from jax.sharding import PartitionSpec as P

MESH = pl.DeviceIdType.MESH
LANES = 128


def partner(step, me, n, turned=0):
    turn, flip = step // 2, lax.rem(step + turned, 2)
    flip = jnp.where(turn == n // 2 - 1, 1 - lax.rem(step, 2), flip)
    half = n // 4
    at = me // 2
    far = at >= half
    w = jnp.where(far, 2 * half - 1 - at, at)
    goal = jnp.where(turn < half, 2 * half - 1 - turn, lax.rem(w + 1 + turn, half))
    goal = jnp.where(far, 2 * half - 1 - goal, goal)
    return goal * 2 + lax.rem(me + flip, 2)


def exchange_kernel(
    n, per_owner, tile, head, ahead_rows,
    tokens, key_weight, value_weight, gates, query,
    kv, outgoing, gate_out, read,
    rows, weights, gate_own, gate_send, gate_in, query_own, query_in, part_send, part_in, mine, theirs, row_in, relayed,
    row_sem, weight_sem, small_sem, send_sem, recv_sem, known_sem, ahead_sem, relay_sent, relay_recv,
    gate_sent, gate_recv, query_sent, query_recv, part_sent, part_recv, pair_sem,
):
    me = lax.axis_index("sp")
    core = lax.axis_index("tp")
    count = rows.shape[0]
    tiles = count // tile
    early = max(tiles - 1, 1)
    columns = weights.shape[3]
    group_heads = columns // head
    owners = group_heads // per_owner
    groups = n // owners

    def group_of(step):
        return partner(step, me // owners, groups, core)

    def load_rows(t):
        span = pl.ds(t * tile, tile - ahead_rows if t == early - 1 else tile)
        return pltpu.make_async_copy(tokens.at[span, :], rows.at[span, :], row_sem.at[t])

    def load_weight(step, which):
        at = pl.ds(pl.multiple_of(group_of(step) * columns, columns), columns)
        source = (key_weight, value_weight)[which]
        return pltpu.make_async_copy(
            source.at[:, at], weights.at[step, which], weight_sem.at[step, which]
        )

    load_query = pltpu.make_async_copy(query, query_own, small_sem.at[0])
    load_gates = pltpu.make_async_copy(gates, gate_own, small_sem.at[1])

    layers = n // 2
    layer = me // 2
    near = layers // 2
    right = layer >= near
    inner = (layer == near - 1) | (layer == near)
    mate = jnp.where(right, me - 2, me + 2)
    ahead_tile = early - 1
    ahead_at = (ahead_tile + 1) * tile - ahead_rows
    ahead_span = pl.ds(ahead_at, ahead_rows)

    def crosses(owner):
        return (owner // 2 >= near) != right

    def is_inner(owner):
        return (owner // 2 == near - 1) | (owner // 2 == near)

    barrier = pltpu.get_barrier_semaphore()
    neighbours = 1 + (layer > 0).astype(jnp.int32) + (layer < layers - 1).astype(jnp.int32)

    def tell_neighbours(sem):
        @pl.when(layer > 0)
        def _():
            pl.semaphore_signal(sem, inc=1, device_id={"sp": me - 2}, device_id_type=MESH)

        @pl.when(layer < layers - 1)
        def _():
            pl.semaphore_signal(sem, inc=1, device_id={"sp": me + 2}, device_id_type=MESH)

        pl.semaphore_signal(
            sem, inc=1, device_id={"sp": me + 1 - 2 * lax.rem(me, 2)}, device_id_type=MESH
        )

    tell_neighbours(barrier)
    pl.semaphore_signal(barrier, inc=1, device_id={"tp": 1 - core}, device_id_type=MESH)
    load_ahead = pltpu.make_async_copy(
        tokens.at[ahead_span, :], rows.at[ahead_span, :], small_sem.at[2]
    )
    load_ahead.start()
    load_rows(0).start()
    load_weight(0, 0).start()
    load_weight(0, 1).start()
    load_gates.start()
    load_query.start()
    for t in range(1, tiles):
        load_rows(t).start()
    send_ahead = pltpu.make_async_remote_copy(
        src_ref=rows.at[ahead_span, :], dst_ref=row_in,
        send_sem=ahead_sem.at[0], recv_sem=ahead_sem.at[1],
        device_id={"sp": mate}, device_id_type=MESH,
    )
    load_ahead.wait()
    pl.semaphore_wait(barrier, neighbours + 1)

    @pl.when(inner)
    def _():
        send_ahead.start()

    tell_neighbours(known_sem.at[0])
    pl.semaphore_wait(known_sem.at[0], neighbours)
    tell_neighbours(known_sem.at[1])

    def query_copy(owner):
        return pltpu.make_async_remote_copy(
            src_ref=query_in.at[me], dst_ref=query_in.at[me],
            send_sem=query_sent.at[owner], recv_sem=query_recv.at[me],
            device_id={"sp": owner}, device_id_type=MESH,
        )

    def gate_copy(owner):
        return pltpu.make_async_remote_copy(
            src_ref=gate_send.at[owner], dst_ref=gate_in.at[me],
            send_sem=gate_sent.at[owner], recv_sem=gate_recv.at[me],
            device_id={"sp": owner}, device_id_type=MESH,
        )

    def part_copy(owner):
        return pltpu.make_async_remote_copy(
            src_ref=part_send.at[owner], dst_ref=part_in.at[me],
            send_sem=part_sent.at[owner], recv_sem=part_recv.at[me],
            device_id={"sp": owner}, device_id_type=MESH,
        )

    def block_copy(owner, t, size=tile):
        return pltpu.make_async_remote_copy(
            src_ref=outgoing.at[owner, :, pl.ds(t * tile, size), :],
            dst_ref=kv.at[:, pl.ds(pl.multiple_of(me * count + t * tile, LANES), size), :],
            send_sem=send_sem.at[owner, t], recv_sem=recv_sem.at[me, t],
            device_id={"sp": owner}, device_id_type=MESH,
        )

    def both_sizes(t, short, act):
        if t == ahead_tile:
            @pl.when(short)
            def _():
                act(tile - ahead_rows)

            @pl.when(jnp.logical_not(short))
            def _():
                act(tile)
        else:
            act(tile)

    def block_own(t):
        return pltpu.make_async_copy(
            outgoing.at[me, :, pl.ds(t * tile, tile), :],
            kv.at[:, pl.ds(pl.multiple_of(me * count + t * tile, tile), tile), :],
            recv_sem.at[me, t],
        )

    def send_block(owner, t):
        @pl.when(owner != me)
        def _():
            both_sizes(t, inner & crosses(owner), lambda size: block_copy(owner, t, size).start())

        @pl.when(owner == me)
        def _():
            block_own(t).start()

    def own_gates(owner, span):
        return jnp.concatenate([gate_own[owner, h, :, span] for h in range(per_owner)], axis=0)

    low = lax.broadcasted_iota(jnp.int32, (tile, LANES), 1) < head

    def open_links():
        pl.semaphore_wait(known_sem.at[1], neighbours)

        @pl.loop(2, layers - 1)
        def _(k):
            tell_neighbours(known_sem.at[k])
            pl.semaphore_wait(known_sem.at[k], neighbours)

    def send_queries():
        load_gates.wait()
        load_query.wait()
        query_in[me] = jnp.concatenate(
            [query_own[...].astype(jnp.float32), jnp.zeros((per_owner, LANES - head), jnp.float32)], axis=1
        ) * (head ** -0.5)

        @pl.loop(0, n - 1)
        def _(k):
            query_copy(partner(k, me, n)).start()

    def send_gates():
        @pl.loop(0, n - 1)
        def _(k):
            owner = partner(k, me, n)
            gate_send[owner] = own_gates(owner, slice(None)).astype(jnp.bfloat16)
            gate_copy(owner).start()

        gate_in[me] = own_gates(me, slice(None)).astype(jnp.bfloat16)

    head_row = lax.broadcasted_iota(jnp.int32, (per_owner, LANES), 0)
    tile_row = lax.broadcasted_iota(jnp.int32, (per_owner, tile), 0)
    lane = lax.broadcasted_iota(jnp.int32, (per_owner, LANES), 1)

    def read_own(owner):
        @pl.when(owner != me)
        def _():
            pltpu.make_async_copy(query_in.at[owner], query_in.at[owner], query_recv.at[owner]).wait()

        asked = query_in[owner]
        queries = [
            jnp.where(head_row == h, asked, 0.0).astype(jnp.bfloat16) for h in range(per_owner)
        ]
        top = jnp.full((per_owner, 1), -1e30, jnp.float32)
        total = jnp.zeros((per_owner, 1), jnp.float32)
        weighted = jnp.zeros((per_owner, LANES), jnp.float32)
        for t in range(tiles):
            span = pl.ds(t * tile, tile)
            blocks = [outgoing[owner, h, span, :] for h in range(per_owner)]
            scores = None
            for h in range(per_owner):
                term = lax.dot_general(
                    queries[h], blocks[h], (((1,), (1,)), ((), ())), preferred_element_type=jnp.float32
                )
                scores = term if scores is None else scores + term
            scores = scores - own_gates(owner, span)
            new_top = jnp.maximum(top, jnp.max(scores, axis=1, keepdims=True))
            scale = jnp.exp(top - new_top)
            probs = jnp.exp(scores - new_top)
            total = total * scale + jnp.sum(probs, axis=1, keepdims=True)
            weighted = weighted * scale
            for h in range(per_owner):
                picked = jnp.where(tile_row == h, probs, 0.0).astype(jnp.bfloat16)
                weighted = weighted + jnp.dot(picked, blocks[h], preferred_element_type=jnp.float32)
            top = new_top
        packed = jnp.where(lane < head // 2, top, jnp.where(lane < head, total, weighted))
        part_send[owner] = packed

        @pl.when(owner != me)
        def _():
            part_copy(owner).start()

    def project(step, first, relays=False):
        group = group_of(step)

        if first:
            for ahead in range(1, min(3, groups)):
                load_weight(ahead, 0).start()
                load_weight(ahead, 1).start()
        else:
            @pl.when(step + 2 < groups)
            def _():
                load_weight(step + 2, 0).start()
                load_weight(step + 2, 1).start()

        load_weight(step, 0).wait()
        load_weight(step, 1).wait()

        def multiply(left, store):
            size = left.shape[0]
            keys = jnp.dot(left, weights[step, 0], preferred_element_type=jnp.float32)
            values = jnp.dot(left, weights[step, 1], preferred_element_type=jnp.float32)
            for pair in range(columns // LANES):
                span = slice(pair * LANES, (pair + 1) * LANES)
                k, v = keys[:, span], values[:, span]
                joined = (
                    jnp.where(low[:size], k, pltpu.roll(v, head, 1)),
                    jnp.where(low[:size], pltpu.roll(k, head, 1), v),
                )
                for half in range(2):
                    local = pair * 2 + half
                    store(
                        group * owners + local // per_owner, local % per_owner, joined[half].astype(jnp.bfloat16)
                    )

        for t in range(tiles):
            if first:
                load_rows(t).wait()

            def keep(owner, h, block):
                outgoing[owner, h, pl.ds(t * tile, tile), :] = block

            multiply(rows[pl.ds(t * tile, tile), :], keep)
            if first and t == 0:
                open_links()
            if t < early:
                for j in range(owners):
                    send_block(group * owners + j, t)
            if first and t == 0:
                send_queries()
        for j in range(owners):
            read_own(group * owners + j)
        if relays:
            @pl.when(inner)
            def _():
                def keep(owner, h, block):
                    relayed[owner, h] = block

                multiply(row_in[...], keep)
                for j in range(owners):
                    owner = group * owners + j

                    @pl.when(owner != me)
                    def _():
                        relay_copy(owner).start()

                    @pl.when(owner == me)
                    def _():
                        kv[:, mate_rows, :] = relayed[owner]

    mate_rows = pl.ds(pl.multiple_of(mate * count + ahead_at, 16), ahead_rows)

    def relay_copy(owner):
        return pltpu.make_async_remote_copy(
            src_ref=relayed.at[owner], dst_ref=kv.at[:, mate_rows, :],
            send_sem=relay_sent.at[owner], recv_sem=relay_recv.at[me],
            device_id={"sp": owner}, device_id_type=MESH,
        )

    project(0, True)
    send_gates()

    def across(step, carry):
        project(step, False)
        return carry

    lax.fori_loop(1, groups // 2, across, 0)

    @pl.when(inner)
    def _():
        send_ahead.wait()

    def along(step, carry):
        project(step, False, True)
        return carry

    lax.fori_loop(groups // 2, groups, along, 0)

    if early < tiles:
        @pl.when(core == 0)
        def _():
            @pl.loop(0, n)
            def _(k):
                for t in range(early, tiles):
                    send_block(partner(k, me, n), t)

    @pl.loop(0, n - 1)
    def _(k):
        source = partner(k, me, n)
        gate_copy(source).wait_send()
        query_copy(source).wait_send()
        pltpu.make_async_copy(gate_in.at[source], gate_in.at[source], gate_recv.at[source]).wait()

    for source in range(n):
        gate_out[:, source * count:(source + 1) * count] = gate_in[source].astype(jnp.float32)

    def merge(one, two):
        top_one, top_two = one[:, :1], two[:, :1]
        joint = jnp.maximum(top_one, top_two)
        both = one * jnp.exp(top_one - joint) + two * jnp.exp(top_two - joint)
        return jnp.where(lane < head // 2, joint, both)

    def gather(k, carry):
        source = partner(n - 2 - k, me, n)
        part_copy(source).wait_send()
        pltpu.make_async_copy(part_in.at[source], part_in.at[source], part_recv.at[source]).wait()
        return merge(carry, part_in[source])

    packed = lax.fori_loop(0, n - 1, gather, part_send[me])
    mine[...] = packed
    swap = pltpu.make_async_remote_copy(
        src_ref=mine, dst_ref=theirs, send_sem=pair_sem.at[0], recv_sem=pair_sem.at[1],
        device_id={"tp": 1 - core}, device_id_type=MESH,
    )
    swap.start()
    swap.wait()
    other = theirs[...]
    joint = merge(jnp.where(core == 0, packed, other), jnp.where(core == 0, other, packed))
    at = head // 2
    answer = joint / joint[:, at:at + 1]
    read[...] = pltpu.roll(answer, head, 1)[:, :head].astype(jnp.bfloat16)

    def settle(t):
        block_own(t).wait()

        @pl.loop(0, n - 1)
        def _(k):
            source = partner(n - 2 - k, me, n)
            both_sizes(t, inner & crosses(source), lambda size: block_copy(source, t, size).wait_send())

            def arrived(size):
                span = pl.ds(t * tile, size)
                pltpu.make_async_copy(kv.at[:, span, :], kv.at[:, span, :], recv_sem.at[source, t]).wait()

            both_sizes(t, is_inner(source) & crosses(source), arrived)

    first_inner = jnp.where(right, near, near - 1) * 2

    @pl.loop(0, 2)
    def _(k):
        source = first_inner + k

        @pl.when(source != me)
        def _():
            pltpu.make_async_copy(
                kv.at[:, ahead_span, :], kv.at[:, ahead_span, :], relay_recv.at[source]
            ).wait()

    @pl.when(inner)
    def _():
        @pl.loop(0, n // 2)
        def _(k):
            owner = jnp.where(right, n // 2, 0) + k

            @pl.when(owner != me)
            def _():
                relay_copy(owner).wait_send()

    for t in range(early):
        settle(t)
    if early < tiles:
        @pl.when(core == 0)
        def _():
            for t in range(early, tiles):
                settle(t)


def rest_kernel(
    n, first_row,
    outgoing, after,
    late,
    send_sem, recv_sem,
):
    me = lax.axis_index("sp")
    size = outgoing.shape[2] - first_row
    held = pl.ds(first_row, size)

    def rows_of(source):
        return pl.ds(pl.multiple_of(source * size, size), size)

    def block_copy(owner):
        return pltpu.make_async_remote_copy(
            src_ref=outgoing.at[owner, :, held, :], dst_ref=late.at[:, rows_of(me), :],
            send_sem=send_sem.at[owner], recv_sem=recv_sem.at[me],
            device_id={"sp": owner}, device_id_type=MESH,
        )

    @pl.when(lax.axis_index("tp") == 1)
    def _():
        barrier = pltpu.get_barrier_semaphore()

        @pl.loop(1, n)
        def _(k):
            pl.semaphore_signal(
                barrier, inc=1, device_id={"sp": lax.rem(me + k, n)}, device_id_type=MESH
            )

        pl.semaphore_wait(barrier, n - 1)

        @pl.loop(0, n - 1)
        def _(k):
            block_copy(partner(k, me, n)).start()

        late[:, rows_of(me), :] = outgoing[me, :, held, :]

        @pl.loop(0, n - 1)
        def _(k):
            source = partner(n - 2 - k, me, n)
            block_copy(source).wait_send()
            pltpu.make_async_copy(
                outgoing.at[0, :, held, :], late.at[:, rows_of(source), :], recv_sem.at[source]
            ).wait()


def finish_kernel(n, first_row, kv, gates, answer, kv_out, gate_out, read, after, sem):
    count = kv.shape[1] // n

    def part(source, start, size, at):
        span = pl.ds(source * count + start, size)
        return pltpu.make_async_copy(kv.at[:, span, :], kv_out.at[:, span, :], sem.at[at])

    small = [
        pltpu.make_async_copy(gates, gate_out, sem.at[2 * n]),
        pltpu.make_async_copy(answer, read, sem.at[2 * n + 1]),
    ]
    early = [part(source, 0, first_row, source) for source in range(n)]
    for copy in early + small:
        copy.start()
    after[...] = jnp.zeros_like(after)
    if first_row < count:
        @pl.when(lax.axis_index("tp") == 0)
        def _():
            late = [part(source, first_row, count - first_row, n + source) for source in range(n)]
            for copy in late:
                copy.start()
            for copy in late:
                copy.wait()
    for copy in early + small:
        copy.wait()


def last_kernel(n, first_row, late, kv, kv_out, sem):
    count = kv_out.shape[1] // n
    size = count - first_row

    @pl.when(lax.axis_index("tp") == 1)
    def _():
        copies = [
            pltpu.make_async_copy(
                late.at[:, pl.ds(source * size, size), :],
                kv_out.at[:, pl.ds(source * count + first_row, size), :],
                sem.at[source],
            )
            for source in range(n)
        ]
        for copy in copies:
            copy.start()
        for copy in copies:
            copy.wait()


def on_device(n, tokens, key_weight, value_weight, cum_gate, query):
    _, _, count, width = tokens.shape
    heads = cum_gate.shape[1]
    per_owner, head = query.shape[1], query.shape[2]
    tile = 256 if count % 256 == 0 else count
    columns = max(per_owner * head, LANES)
    groups = heads * head // columns
    tiles = count // tile
    ahead_rows = tile // 8
    any_space = pl.BlockSpec(memory_space=pl.ANY)
    outside = pl.BlockSpec(memory_space=pltpu.HBM)
    vmem = pl.BlockSpec(memory_space=pltpu.VMEM)
    kv, outgoing, gates, answer = pl.pallas_call(
        functools.partial(exchange_kernel, n, per_owner, tile, head, ahead_rows),
        name="exchange",
        out_shape=(
            pltpu.VMEM((per_owner, n * count, 2 * head), jnp.bfloat16),
            pltpu.VMEM((n, per_owner, count, 2 * head), jnp.bfloat16),
            pltpu.VMEM((per_owner, n * count), jnp.float32),
            pltpu.VMEM((per_owner, head), jnp.bfloat16),
        ),
        in_specs=[outside] * 5,
        out_specs=(vmem, vmem, vmem, vmem),
        scratch_shapes=[
            pltpu.VMEM((count, width), jnp.bfloat16),
            pltpu.VMEM((groups, 2, width, columns), jnp.bfloat16),
            pltpu.VMEM((n, per_owner, 1, count), jnp.float32),
            pltpu.VMEM((n, per_owner, count), jnp.bfloat16),
            pltpu.VMEM((n, per_owner, count), jnp.bfloat16),
            pltpu.VMEM((per_owner, head), jnp.bfloat16),
            pltpu.VMEM((n, per_owner, LANES), jnp.float32),
            pltpu.VMEM((n, per_owner, LANES), jnp.float32),
            pltpu.VMEM((n, per_owner, LANES), jnp.float32),
            pltpu.VMEM((per_owner, LANES), jnp.float32),
            pltpu.VMEM((per_owner, LANES), jnp.float32),
            pltpu.VMEM((ahead_rows, width), jnp.bfloat16),
            pltpu.VMEM((n, per_owner, ahead_rows, 2 * head), jnp.bfloat16),
            pltpu.SemaphoreType.DMA((tiles,)),
            pltpu.SemaphoreType.DMA((groups, 2)),
            pltpu.SemaphoreType.DMA((3,)),
            pltpu.SemaphoreType.DMA((n, tiles)),
            pltpu.SemaphoreType.DMA((n, tiles)),
            pltpu.SemaphoreType.REGULAR((n // 2,)),
            pltpu.SemaphoreType.DMA((2,)),
            pltpu.SemaphoreType.DMA((n,)),
            pltpu.SemaphoreType.DMA((n,)),
            pltpu.SemaphoreType.DMA((n,)),
            pltpu.SemaphoreType.DMA((n,)),
            pltpu.SemaphoreType.DMA((n,)),
            pltpu.SemaphoreType.DMA((n,)),
            pltpu.SemaphoreType.DMA((n,)),
            pltpu.SemaphoreType.DMA((n,)),
            pltpu.SemaphoreType.DMA((2,)),
        ],
        compiler_params=pltpu.CompilerParams(
            collective_id=0, has_side_effects=True, vmem_limit_bytes=48 * 1024 * 1024
        ),
    )(
        tokens.reshape(count, width),
        key_weight,
        value_weight,
        cum_gate.reshape(n, per_owner, 1, count),
        query.reshape(per_owner, head),
    )
    first_row = max(tiles - 1, 1) * tile
    whole = jax.ShapeDtypeStruct((per_owner, n * count, 2 * head), jnp.bfloat16)
    kv_out, gate_out, read, after = pl.pallas_call(
        functools.partial(finish_kernel, n, first_row),
        name="finish",
        out_shape=(
            whole,
            jax.ShapeDtypeStruct((per_owner, n * count), jnp.float32),
            jax.ShapeDtypeStruct((per_owner, head), jnp.bfloat16),
            pltpu.VMEM((8, LANES), jnp.float32),
        ),
        in_specs=[vmem, vmem, vmem],
        out_specs=(any_space, any_space, any_space, vmem),
        scratch_shapes=[pltpu.SemaphoreType.DMA((2 * n + 2,))],
        compiler_params=pltpu.CompilerParams(vmem_limit_bytes=16 * 1024 * 1024),
    )(kv, gates, answer)
    if first_row < count:
        late = pl.pallas_call(
            functools.partial(rest_kernel, n, first_row),
            name="rest",
            out_shape=pltpu.VMEM((per_owner, n * (count - first_row), 2 * head), jnp.bfloat16),
            in_specs=[vmem, vmem],
            out_specs=vmem,
            scratch_shapes=[pltpu.SemaphoreType.DMA((n,)), pltpu.SemaphoreType.DMA((n,))],
            compiler_params=pltpu.CompilerParams(
                collective_id=1, has_side_effects=True, vmem_limit_bytes=16 * 1024 * 1024
            ),
        )(outgoing, after)
        kv_out = pl.pallas_call(
            functools.partial(last_kernel, n, first_row),
            name="last",
            out_shape=whole,
            in_specs=[vmem, any_space],
            out_specs=any_space,
            input_output_aliases={1: 0},
            scratch_shapes=[pltpu.SemaphoreType.DMA((n,))],
            compiler_params=pltpu.CompilerParams(vmem_limit_bytes=16 * 1024 * 1024),
        )(late, kv_out)
    return kv_out[None], gate_out[None], read[None]


def solution(mesh):
    placed = (P("gr", "tp", "sp", None), P(), P(), P("gr", None, "tp", "sp"), P("gr", "sp", None))
    return jax.shard_map(
        functools.partial(on_device, mesh.shape["sp"]),
        mesh=mesh,
        in_specs=placed,
        out_specs=(P("gr", "sp", "tp", None), P("gr", "sp", "tp"), P("gr", "sp", None)),
        check_vma=False,
    )
```

```python
import functools

import jax
import jax.numpy as jnp
from jax import lax
from jax.experimental import pallas as pl
from jax.experimental.pallas import tpu as pltpu
from jax.sharding import PartitionSpec as P

MESH = pl.DeviceIdType.MESH
LANES = 128


def partner(step, me, n, turned=0):
    turn, flip = step // 2, lax.rem(step + turned, 2)
    flip = jnp.where(turn == n // 2 - 1, 1 - lax.rem(step, 2), flip)
    half = n // 4
    at = me // 2
    far = at >= half
    w = jnp.where(far, 2 * half - 1 - at, at)
    goal = jnp.where(turn < half, 2 * half - 1 - turn, lax.rem(w + 1 + turn, half))
    goal = jnp.where(far, 2 * half - 1 - goal, goal)
    return goal * 2 + lax.rem(me + flip, 2)


def exchange_kernel(
    n, per_owner, tile, head, ahead_rows,
    tokens, key_weight, value_weight, gates, query,
    kv, outgoing, gate_out, read,
    rows, weights, gate_own, gate_send, gate_in, query_own, query_in, part_send, part_in, mine, theirs, row_in, relayed,
    row_sem, weight_sem, small_sem, send_sem, recv_sem, known_sem, ahead_sem, relay_sent, relay_recv,
    gate_sent, gate_recv, query_sent, query_recv, part_sent, part_recv, pair_sem,
):
    me = lax.axis_index("sp")
    core = lax.axis_index("tp")
    count = rows.shape[0]
    tiles = count // tile
    early = max(tiles - 1, 1)
    columns = weights.shape[3]
    group_heads = columns // head
    owners = group_heads // per_owner
    groups = n // owners

    def group_of(step):
        return partner(step, me // owners, groups, core)

    def load_rows(t):
        span = pl.ds(t * tile, tile - ahead_rows if t == early - 1 else tile)
        return pltpu.make_async_copy(tokens.at[span, :], rows.at[span, :], row_sem.at[t])

    def load_weight(step, which):
        at = pl.ds(pl.multiple_of(group_of(step) * columns, columns), columns)
        source = (key_weight, value_weight)[which]
        return pltpu.make_async_copy(
            source.at[:, at], weights.at[step, which], weight_sem.at[step, which]
        )

    load_query = pltpu.make_async_copy(query, query_own, small_sem.at[0])
    load_gates = pltpu.make_async_copy(gates, gate_own, small_sem.at[1])

    layers = n // 2
    layer = me // 2
    near = layers // 2
    right = layer >= near
    inner = (layer == near - 1) | (layer == near)
    mate = jnp.where(right, me - 2, me + 2)
    ahead_tile = early - 1
    ahead_at = (ahead_tile + 1) * tile - ahead_rows
    ahead_span = pl.ds(ahead_at, ahead_rows)

    def crosses(owner):
        return (owner // 2 >= near) != right

    def is_inner(owner):
        return (owner // 2 == near - 1) | (owner // 2 == near)

    barrier = pltpu.get_barrier_semaphore()
    neighbours = 1 + (layer > 0).astype(jnp.int32) + (layer < layers - 1).astype(jnp.int32)

    def tell_neighbours(sem):
        @pl.when(layer > 0)
        def _():
            pl.semaphore_signal(sem, inc=1, device_id={"sp": me - 2}, device_id_type=MESH)

        @pl.when(layer < layers - 1)
        def _():
            pl.semaphore_signal(sem, inc=1, device_id={"sp": me + 2}, device_id_type=MESH)

        pl.semaphore_signal(
            sem, inc=1, device_id={"sp": me + 1 - 2 * lax.rem(me, 2)}, device_id_type=MESH
        )

    side = lax.rem(me, 2)
    outward = jnp.where(right, me + 2, me - 2)
    inward = jnp.where(right, me - 2, me + 2)
    has_outward = jnp.logical_not((layer == 0) | (layer == layers - 1))

    def tell(sem, to):
        pl.semaphore_signal(sem, inc=1, device_id=to, device_id_type=MESH)

    @pl.when(inner)
    def _():
        tell(barrier, {"sp": mate})

    @pl.when(side == 0)
    def _():
        tell(barrier, {"sp": me + 1})

    @pl.when(core == 0)
    def _():
        tell(barrier, {"tp": 1 - core})

    @pl.when(has_outward)
    def _():
        tell(barrier, {"sp": outward})

    load_ahead = pltpu.make_async_copy(
        tokens.at[ahead_span, :], rows.at[ahead_span, :], small_sem.at[2]
    )
    load_ahead.start()
    load_rows(0).start()
    load_weight(0, 0).start()
    load_weight(0, 1).start()
    load_gates.start()
    load_query.start()
    for t in range(1, tiles):
        load_rows(t).start()
    send_ahead = pltpu.make_async_remote_copy(
        src_ref=rows.at[ahead_span, :], dst_ref=row_in,
        send_sem=ahead_sem.at[0], recv_sem=ahead_sem.at[1],
        device_id={"sp": mate}, device_id_type=MESH,
    )
    load_ahead.wait()
    pl.semaphore_wait(barrier, 1 + side + core)

    @pl.when(inner)
    def _():
        send_ahead.start()

    @pl.when(jnp.logical_not(inner))
    def _():
        tell(known_sem.at[0], {"sp": inward})

    @pl.when(side == 1)
    def _():
        tell(known_sem.at[0], {"sp": me - 1})

    @pl.when(core == 1)
    def _():
        tell(known_sem.at[0], {"tp": 1 - core})

    replies = has_outward.astype(jnp.int32) + 2 - side - core

    @pl.when(replies > 0)
    def _():
        pl.semaphore_wait(known_sem.at[0], replies)

    tell_neighbours(known_sem.at[1])
    pl.semaphore_wait(known_sem.at[1], neighbours)
    tell_neighbours(known_sem.at[2])

    def query_copy(owner):
        return pltpu.make_async_remote_copy(
            src_ref=query_in.at[me], dst_ref=query_in.at[me],
            send_sem=query_sent.at[owner], recv_sem=query_recv.at[me],
            device_id={"sp": owner}, device_id_type=MESH,
        )

    def gate_copy(owner):
        return pltpu.make_async_remote_copy(
            src_ref=gate_send.at[owner], dst_ref=gate_in.at[me],
            send_sem=gate_sent.at[owner], recv_sem=gate_recv.at[me],
            device_id={"sp": owner}, device_id_type=MESH,
        )

    def part_copy(owner):
        return pltpu.make_async_remote_copy(
            src_ref=part_send.at[owner], dst_ref=part_in.at[me],
            send_sem=part_sent.at[owner], recv_sem=part_recv.at[me],
            device_id={"sp": owner}, device_id_type=MESH,
        )

    def block_copy(owner, t, size=tile):
        return pltpu.make_async_remote_copy(
            src_ref=outgoing.at[owner, :, pl.ds(t * tile, size), :],
            dst_ref=kv.at[:, pl.ds(pl.multiple_of(me * count + t * tile, LANES), size), :],
            send_sem=send_sem.at[owner, t], recv_sem=recv_sem.at[me, t],
            device_id={"sp": owner}, device_id_type=MESH,
        )

    def both_sizes(t, short, act):
        if t == ahead_tile:
            @pl.when(short)
            def _():
                act(tile - ahead_rows)

            @pl.when(jnp.logical_not(short))
            def _():
                act(tile)
        else:
            act(tile)

    def block_own(t):
        return pltpu.make_async_copy(
            outgoing.at[me, :, pl.ds(t * tile, tile), :],
            kv.at[:, pl.ds(pl.multiple_of(me * count + t * tile, tile), tile), :],
            recv_sem.at[me, t],
        )

    def send_block(owner, t):
        @pl.when(owner != me)
        def _():
            both_sizes(t, inner & crosses(owner), lambda size: block_copy(owner, t, size).start())

        @pl.when(owner == me)
        def _():
            block_own(t).start()

    def own_gates(owner, span):
        return jnp.concatenate([gate_own[owner, h, :, span] for h in range(per_owner)], axis=0)

    low = lax.broadcasted_iota(jnp.int32, (tile, LANES), 1) < head

    def open_links(first_round, last_round):
        for at in range(first_round - 1, last_round):
            pl.semaphore_wait(known_sem.at[at], neighbours)
            if at + 1 < layers:
                tell_neighbours(known_sem.at[at + 1])

    def send_queries():
        load_gates.wait()
        load_query.wait()
        wide = jnp.concatenate(
            [query_own[...].astype(jnp.float32), jnp.zeros((per_owner, LANES - head), jnp.float32)], axis=1
        ) * (head ** -0.5)
        query_in[me] = wide.astype(jnp.bfloat16)

        @pl.loop(0, n - 1)
        def _(k):
            query_copy(partner(k, me, n)).start()

    def send_gates():
        @pl.loop(0, n - 1)
        def _(k):
            owner = partner(k, me, n)
            gate_send[owner] = own_gates(owner, slice(None)).astype(jnp.bfloat16)
            gate_copy(owner).start()

        gate_in[me] = own_gates(me, slice(None)).astype(jnp.bfloat16)

    head_row = lax.broadcasted_iota(jnp.int32, (per_owner, LANES), 0)
    tile_row = lax.broadcasted_iota(jnp.int32, (per_owner, tile), 0)
    lane = lax.broadcasted_iota(jnp.int32, (per_owner, LANES), 1)

    def read_own(owner):
        @pl.when(owner != me)
        def _():
            pltpu.make_async_copy(query_in.at[owner], query_in.at[owner], query_recv.at[owner]).wait()

        asked = query_in[owner].astype(jnp.float32)
        queries = [
            jnp.where(head_row == h, asked, 0.0).astype(jnp.bfloat16) for h in range(per_owner)
        ]
        top = jnp.full((per_owner, 1), -1e30, jnp.float32)
        total = jnp.zeros((per_owner, 1), jnp.float32)
        weighted = jnp.zeros((per_owner, LANES), jnp.float32)
        for t in range(tiles):
            span = pl.ds(t * tile, tile)
            blocks = [outgoing[owner, h, span, :] for h in range(per_owner)]
            scores = None
            for h in range(per_owner):
                term = lax.dot_general(
                    queries[h], blocks[h], (((1,), (1,)), ((), ())), preferred_element_type=jnp.float32
                )
                scores = term if scores is None else scores + term
            scores = scores - own_gates(owner, span)
            new_top = jnp.maximum(top, jnp.max(scores, axis=1, keepdims=True))
            scale = jnp.exp(top - new_top)
            probs = jnp.exp(scores - new_top)
            total = total * scale + jnp.sum(probs, axis=1, keepdims=True)
            weighted = weighted * scale
            for h in range(per_owner):
                picked = jnp.where(tile_row == h, probs, 0.0).astype(jnp.bfloat16)
                weighted = weighted + jnp.dot(picked, blocks[h], preferred_element_type=jnp.float32)
            top = new_top
        packed = jnp.where(lane < head // 2, top, jnp.where(lane < head, total, weighted))
        part_send[owner] = packed

        @pl.when(owner != me)
        def _():
            part_copy(owner).start()

    def project(step, first, relays=False):
        group = group_of(step)

        if first:
            for ahead in range(1, min(3, groups)):
                load_weight(ahead, 0).start()
                load_weight(ahead, 1).start()
        else:
            @pl.when(step + 2 < groups)
            def _():
                load_weight(step + 2, 0).start()
                load_weight(step + 2, 1).start()

        load_weight(step, 0).wait()
        load_weight(step, 1).wait()

        def multiply(left, store):
            size = left.shape[0]
            keys = jnp.dot(left, weights[step, 0], preferred_element_type=jnp.float32)
            values = jnp.dot(left, weights[step, 1], preferred_element_type=jnp.float32)
            for pair in range(columns // LANES):
                span = slice(pair * LANES, (pair + 1) * LANES)
                k, v = keys[:, span], values[:, span]
                joined = (
                    jnp.where(low[:size], k, pltpu.roll(v, head, 1)),
                    jnp.where(low[:size], pltpu.roll(k, head, 1), v),
                )
                for half in range(2):
                    local = pair * 2 + half
                    store(
                        group * owners + local // per_owner, local % per_owner, joined[half].astype(jnp.bfloat16)
                    )

        for t in range(tiles):
            if first:
                load_rows(t).wait()

            def keep(owner, h, block):
                outgoing[owner, h, pl.ds(t * tile, tile), :] = block

            multiply(rows[pl.ds(t * tile, tile), :], keep)
            if first and t == 0:
                open_links(3, near + 1)

                @pl.when(inner)
                def _():
                    for j in range(owners):
                        send_block(group * owners + j, t)

                open_links(near + 2, layers)

                @pl.when(jnp.logical_not(inner))
                def _():
                    for j in range(owners):
                        send_block(group * owners + j, t)
            elif t < early:
                for j in range(owners):
                    send_block(group * owners + j, t)
            if first and t == 0:
                send_queries()
        for j in range(owners):
            read_own(group * owners + j)
        if relays:
            @pl.when(inner)
            def _():
                def keep(owner, h, block):
                    relayed[owner, h] = block

                multiply(row_in[...], keep)
                for j in range(owners):
                    owner = group * owners + j

                    @pl.when(owner != me)
                    def _():
                        relay_copy(owner).start()

                    @pl.when(owner == me)
                    def _():
                        kv[:, mate_rows, :] = relayed[owner]

    mate_rows = pl.ds(pl.multiple_of(mate * count + ahead_at, 16), ahead_rows)

    def relay_copy(owner):
        return pltpu.make_async_remote_copy(
            src_ref=relayed.at[owner], dst_ref=kv.at[:, mate_rows, :],
            send_sem=relay_sent.at[owner], recv_sem=relay_recv.at[me],
            device_id={"sp": owner}, device_id_type=MESH,
        )

    project(0, True)
    send_gates()

    def across(step, carry):
        project(step, False)
        return carry

    lax.fori_loop(1, groups // 2, across, 0)

    @pl.when(inner)
    def _():
        send_ahead.wait()

    def along(step, carry):
        project(step, False, True)
        return carry

    lax.fori_loop(groups // 2, groups, along, 0)

    if early < tiles:
        @pl.when(core == 0)
        def _():
            @pl.loop(0, n)
            def _(k):
                for t in range(early, tiles):
                    send_block(partner(k, me, n), t)

    @pl.loop(0, n - 1)
    def _(k):
        source = partner(k, me, n)
        gate_copy(source).wait_send()
        query_copy(source).wait_send()
        pltpu.make_async_copy(gate_in.at[source], gate_in.at[source], gate_recv.at[source]).wait()

    for source in range(n):
        gate_out[:, source * count:(source + 1) * count] = gate_in[source].astype(jnp.float32)

    def merge(one, two):
        top_one, top_two = one[:, :1], two[:, :1]
        joint = jnp.maximum(top_one, top_two)
        both = one * jnp.exp(top_one - joint) + two * jnp.exp(top_two - joint)
        return jnp.where(lane < head // 2, joint, both)

    def gather(k, carry):
        source = partner(n - 2 - k, me, n)
        part_copy(source).wait_send()
        pltpu.make_async_copy(part_in.at[source], part_in.at[source], part_recv.at[source]).wait()
        return merge(carry, part_in[source])

    packed = lax.fori_loop(0, n - 1, gather, part_send[me])
    mine[...] = packed
    swap = pltpu.make_async_remote_copy(
        src_ref=mine, dst_ref=theirs, send_sem=pair_sem.at[0], recv_sem=pair_sem.at[1],
        device_id={"tp": 1 - core}, device_id_type=MESH,
    )
    swap.start()
    swap.wait()
    other = theirs[...]
    joint = merge(jnp.where(core == 0, packed, other), jnp.where(core == 0, other, packed))
    at = head // 2
    answer = joint / joint[:, at:at + 1]
    read[...] = pltpu.roll(answer, head, 1)[:, :head].astype(jnp.bfloat16)

    def settle(t):
        block_own(t).wait()

        @pl.loop(0, n - 1)
        def _(k):
            source = partner(n - 2 - k, me, n)
            both_sizes(t, inner & crosses(source), lambda size: block_copy(source, t, size).wait_send())

            def arrived(size):
                span = pl.ds(t * tile, size)
                pltpu.make_async_copy(kv.at[:, span, :], kv.at[:, span, :], recv_sem.at[source, t]).wait()

            both_sizes(t, is_inner(source) & crosses(source), arrived)

    first_inner = jnp.where(right, near, near - 1) * 2

    @pl.loop(0, 2)
    def _(k):
        source = first_inner + k

        @pl.when(source != me)
        def _():
            pltpu.make_async_copy(
                kv.at[:, ahead_span, :], kv.at[:, ahead_span, :], relay_recv.at[source]
            ).wait()

    @pl.when(inner)
    def _():
        @pl.loop(0, n // 2)
        def _(k):
            owner = jnp.where(right, n // 2, 0) + k

            @pl.when(owner != me)
            def _():
                relay_copy(owner).wait_send()

    for t in range(early):
        settle(t)
    if early < tiles:
        @pl.when(core == 0)
        def _():
            for t in range(early, tiles):
                settle(t)


def rest_kernel(
    n, first_row,
    outgoing, after,
    late,
    send_sem, recv_sem,
):
    me = lax.axis_index("sp")
    size = outgoing.shape[2] - first_row
    held = pl.ds(first_row, size)

    def rows_of(source):
        return pl.ds(pl.multiple_of(source * size, size), size)

    def block_copy(owner):
        return pltpu.make_async_remote_copy(
            src_ref=outgoing.at[owner, :, held, :], dst_ref=late.at[:, rows_of(me), :],
            send_sem=send_sem.at[owner], recv_sem=recv_sem.at[me],
            device_id={"sp": owner}, device_id_type=MESH,
        )

    @pl.when(lax.axis_index("tp") == 1)
    def _():
        barrier = pltpu.get_barrier_semaphore()

        @pl.loop(1, n)
        def _(k):
            pl.semaphore_signal(
                barrier, inc=1, device_id={"sp": lax.rem(me + k, n)}, device_id_type=MESH
            )

        pl.semaphore_wait(barrier, n - 1)

        @pl.loop(0, n - 1)
        def _(k):
            block_copy(partner(k, me, n)).start()

        late[:, rows_of(me), :] = outgoing[me, :, held, :]

        @pl.loop(0, n - 1)
        def _(k):
            source = partner(n - 2 - k, me, n)
            block_copy(source).wait_send()
            pltpu.make_async_copy(
                outgoing.at[0, :, held, :], late.at[:, rows_of(source), :], recv_sem.at[source]
            ).wait()


def finish_kernel(n, first_row, kv, gates, answer, kv_out, gate_out, read, after, sem):
    count = kv.shape[1] // n

    def part(source, start, size, at):
        span = pl.ds(source * count + start, size)
        return pltpu.make_async_copy(kv.at[:, span, :], kv_out.at[:, span, :], sem.at[at])

    small = [
        pltpu.make_async_copy(gates, gate_out, sem.at[2 * n]),
        pltpu.make_async_copy(answer, read, sem.at[2 * n + 1]),
    ]
    early = [part(source, 0, first_row, source) for source in range(n)]
    for copy in early + small:
        copy.start()
    after[...] = jnp.zeros_like(after)
    if first_row < count:
        @pl.when(lax.axis_index("tp") == 0)
        def _():
            late = [part(source, first_row, count - first_row, n + source) for source in range(n)]
            for copy in late:
                copy.start()
            for copy in late:
                copy.wait()
    for copy in early + small:
        copy.wait()


def last_kernel(n, first_row, late, kv, kv_out, sem):
    count = kv_out.shape[1] // n
    size = count - first_row

    @pl.when(lax.axis_index("tp") == 1)
    def _():
        copies = [
            pltpu.make_async_copy(
                late.at[:, pl.ds(source * size, size), :],
                kv_out.at[:, pl.ds(source * count + first_row, size), :],
                sem.at[source],
            )
            for source in range(n)
        ]
        for copy in copies:
            copy.start()
        for copy in copies:
            copy.wait()


def on_device(n, tokens, key_weight, value_weight, cum_gate, query):
    _, _, count, width = tokens.shape
    heads = cum_gate.shape[1]
    per_owner, head = query.shape[1], query.shape[2]
    tile = 256 if count % 256 == 0 else count
    columns = max(per_owner * head, LANES)
    groups = heads * head // columns
    tiles = count // tile
    ahead_rows = tile // 8
    any_space = pl.BlockSpec(memory_space=pl.ANY)
    outside = pl.BlockSpec(memory_space=pltpu.HBM)
    vmem = pl.BlockSpec(memory_space=pltpu.VMEM)
    kv, outgoing, gates, answer = pl.pallas_call(
        functools.partial(exchange_kernel, n, per_owner, tile, head, ahead_rows),
        name="exchange",
        out_shape=(
            pltpu.VMEM((per_owner, n * count, 2 * head), jnp.bfloat16),
            pltpu.VMEM((n, per_owner, count, 2 * head), jnp.bfloat16),
            pltpu.VMEM((per_owner, n * count), jnp.float32),
            pltpu.VMEM((per_owner, head), jnp.bfloat16),
        ),
        in_specs=[outside] * 5,
        out_specs=(vmem, vmem, vmem, vmem),
        scratch_shapes=[
            pltpu.VMEM((count, width), jnp.bfloat16),
            pltpu.VMEM((groups, 2, width, columns), jnp.bfloat16),
            pltpu.VMEM((n, per_owner, 1, count), jnp.float32),
            pltpu.VMEM((n, per_owner, count), jnp.bfloat16),
            pltpu.VMEM((n, per_owner, count), jnp.bfloat16),
            pltpu.VMEM((per_owner, head), jnp.bfloat16),
            pltpu.VMEM((n, per_owner, LANES), jnp.bfloat16),
            pltpu.VMEM((n, per_owner, LANES), jnp.float32),
            pltpu.VMEM((n, per_owner, LANES), jnp.float32),
            pltpu.VMEM((per_owner, LANES), jnp.float32),
            pltpu.VMEM((per_owner, LANES), jnp.float32),
            pltpu.VMEM((ahead_rows, width), jnp.bfloat16),
            pltpu.VMEM((n, per_owner, ahead_rows, 2 * head), jnp.bfloat16),
            pltpu.SemaphoreType.DMA((tiles,)),
            pltpu.SemaphoreType.DMA((groups, 2)),
            pltpu.SemaphoreType.DMA((3,)),
            pltpu.SemaphoreType.DMA((n, tiles)),
            pltpu.SemaphoreType.DMA((n, tiles)),
            pltpu.SemaphoreType.REGULAR((n // 2,)),
            pltpu.SemaphoreType.DMA((2,)),
            pltpu.SemaphoreType.DMA((n,)),
            pltpu.SemaphoreType.DMA((n,)),
            pltpu.SemaphoreType.DMA((n,)),
            pltpu.SemaphoreType.DMA((n,)),
            pltpu.SemaphoreType.DMA((n,)),
            pltpu.SemaphoreType.DMA((n,)),
            pltpu.SemaphoreType.DMA((n,)),
            pltpu.SemaphoreType.DMA((n,)),
            pltpu.SemaphoreType.DMA((2,)),
        ],
        compiler_params=pltpu.CompilerParams(
            collective_id=0, has_side_effects=True, vmem_limit_bytes=48 * 1024 * 1024
        ),
    )(
        tokens.reshape(count, width),
        key_weight,
        value_weight,
        cum_gate.reshape(n, per_owner, 1, count),
        query.reshape(per_owner, head),
    )
    first_row = max(tiles - 1, 1) * tile
    whole = jax.ShapeDtypeStruct((per_owner, n * count, 2 * head), jnp.bfloat16)
    kv_out, gate_out, read, after = pl.pallas_call(
        functools.partial(finish_kernel, n, first_row),
        name="finish",
        out_shape=(
            whole,
            jax.ShapeDtypeStruct((per_owner, n * count), jnp.float32),
            jax.ShapeDtypeStruct((per_owner, head), jnp.bfloat16),
            pltpu.VMEM((8, LANES), jnp.float32),
        ),
        in_specs=[vmem, vmem, vmem],
        out_specs=(any_space, any_space, any_space, vmem),
        scratch_shapes=[pltpu.SemaphoreType.DMA((2 * n + 2,))],
        compiler_params=pltpu.CompilerParams(vmem_limit_bytes=16 * 1024 * 1024),
    )(kv, gates, answer)
    if first_row < count:
        late = pl.pallas_call(
            functools.partial(rest_kernel, n, first_row),
            name="rest",
            out_shape=pltpu.VMEM((per_owner, n * (count - first_row), 2 * head), jnp.bfloat16),
            in_specs=[vmem, vmem],
            out_specs=vmem,
            scratch_shapes=[pltpu.SemaphoreType.DMA((n,)), pltpu.SemaphoreType.DMA((n,))],
            compiler_params=pltpu.CompilerParams(
                collective_id=1, has_side_effects=True, vmem_limit_bytes=16 * 1024 * 1024
            ),
        )(outgoing, after)
        kv_out = pl.pallas_call(
            functools.partial(last_kernel, n, first_row),
            name="last",
            out_shape=whole,
            in_specs=[vmem, any_space],
            out_specs=any_space,
            input_output_aliases={1: 0},
            scratch_shapes=[pltpu.SemaphoreType.DMA((n,))],
            compiler_params=pltpu.CompilerParams(vmem_limit_bytes=16 * 1024 * 1024),
        )(late, kv_out)
    return kv_out[None], gate_out[None], read[None]


def solution(mesh):
    placed = (P("gr", "tp", "sp", None), P(), P(), P("gr", None, "tp", "sp"), P("gr", "sp", None))
    return jax.shard_map(
        functools.partial(on_device, mesh.shape["sp"]),
        mesh=mesh,
        in_specs=placed,
        out_specs=(P("gr", "sp", "tp", None), P("gr", "sp", "tp"), P("gr", "sp", None)),
        check_vma=False,
    )
```

```python
import functools

import jax
import jax.numpy as jnp
from jax import lax
from jax.experimental import pallas as pl
from jax.experimental.pallas import tpu as pltpu
from jax.sharding import PartitionSpec as P

MESH = pl.DeviceIdType.MESH
LANES = 128


def partner(step, me, n, turned=0):
    turn, flip = step // 2, lax.rem(step + turned, 2)
    flip = jnp.where(turn == n // 2 - 1, 1 - lax.rem(step, 2), flip)
    half = n // 4
    at = me // 2
    far = at >= half
    w = jnp.where(far, 2 * half - 1 - at, at)
    goal = jnp.where(turn < half, 2 * half - 1 - turn, lax.rem(w + 1 + turn, half))
    goal = jnp.where(far, 2 * half - 1 - goal, goal)
    return goal * 2 + lax.rem(me + flip, 2)


def exchange_kernel(
    n, per_owner, tile, head, ahead_rows,
    tokens, key_weight, value_weight, gates, query,
    kv, outgoing, gate_out, read,
    rows, weights, gate_own, gate_send, gate_in, query_own, query_in, part_send, part_in, mine, theirs, row_in, relayed,
    row_sem, weight_sem, small_sem, send_sem, recv_sem, known_sem, ahead_sem, relay_sent, relay_recv,
    gate_sent, gate_recv, query_sent, query_recv, part_sent, part_recv, pair_sem,
):
    me = lax.axis_index("sp")
    core = lax.axis_index("tp")
    count = rows.shape[0]
    tiles = count // tile
    early = max(tiles - 1, 1)
    columns = weights.shape[3]
    group_heads = columns // head
    owners = group_heads // per_owner
    groups = n // owners

    def group_of(step):
        return partner(step, me // owners, groups, core)

    def load_rows(t):
        span = pl.ds(t * tile, tile - ahead_rows if t == early - 1 else tile)
        return pltpu.make_async_copy(tokens.at[span, :], rows.at[span, :], row_sem.at[t])

    def load_weight(step, which):
        at = pl.ds(pl.multiple_of(group_of(step) * columns, columns), columns)
        source = (key_weight, value_weight)[which]
        return pltpu.make_async_copy(
            source.at[:, at], weights.at[step, which], weight_sem.at[step, which]
        )

    load_query = pltpu.make_async_copy(query, query_own, small_sem.at[0])
    load_gates = pltpu.make_async_copy(gates, gate_own, small_sem.at[1])

    layers = n // 2
    layer = me // 2
    near = layers // 2
    right = layer >= near
    inner = (layer == near - 1) | (layer == near)
    mate = jnp.where(right, me - 2, me + 2)
    ahead_tile = early - 1
    ahead_at = (ahead_tile + 1) * tile - ahead_rows
    ahead_span = pl.ds(ahead_at, ahead_rows)

    def crosses(owner):
        return (owner // 2 >= near) != right

    def is_inner(owner):
        return (owner // 2 == near - 1) | (owner // 2 == near)

    barrier = pltpu.get_barrier_semaphore()
    neighbours = 1 + (layer > 0).astype(jnp.int32) + (layer < layers - 1).astype(jnp.int32)

    def tell_neighbours(sem):
        @pl.when(layer > 0)
        def _():
            pl.semaphore_signal(sem, inc=1, device_id={"sp": me - 2}, device_id_type=MESH)

        @pl.when(layer < layers - 1)
        def _():
            pl.semaphore_signal(sem, inc=1, device_id={"sp": me + 2}, device_id_type=MESH)

        pl.semaphore_signal(
            sem, inc=1, device_id={"sp": me + 1 - 2 * lax.rem(me, 2)}, device_id_type=MESH
        )

    side = lax.rem(me, 2)
    outward = jnp.where(right, me + 2, me - 2)
    inward = jnp.where(right, me - 2, me + 2)
    has_outward = jnp.logical_not((layer == 0) | (layer == layers - 1))

    def tell(sem, to):
        pl.semaphore_signal(sem, inc=1, device_id=to, device_id_type=MESH)

    @pl.when(inner)
    def _():
        tell(barrier, {"sp": mate})

    @pl.when(side == 0)
    def _():
        tell(barrier, {"sp": me + 1})

    @pl.when(core == 0)
    def _():
        tell(barrier, {"tp": 1 - core})

    @pl.when(has_outward)
    def _():
        tell(barrier, {"sp": outward})

    load_ahead = pltpu.make_async_copy(
        tokens.at[ahead_span, :], rows.at[ahead_span, :], small_sem.at[2]
    )
    load_ahead.start()
    load_rows(0).start()
    load_weight(0, 0).start()
    load_weight(0, 1).start()
    load_gates.start()
    load_query.start()
    for t in range(1, tiles):
        load_rows(t).start()
    send_ahead = pltpu.make_async_remote_copy(
        src_ref=rows.at[ahead_span, :], dst_ref=row_in,
        send_sem=ahead_sem.at[0], recv_sem=ahead_sem.at[1],
        device_id={"sp": mate}, device_id_type=MESH,
    )
    load_ahead.wait()
    pl.semaphore_wait(barrier, 1 + side + core)

    @pl.when(inner)
    def _():
        send_ahead.start()

    @pl.when(jnp.logical_not(inner))
    def _():
        tell(known_sem.at[0], {"sp": inward})

    @pl.when(side == 1)
    def _():
        tell(known_sem.at[0], {"sp": me - 1})

    @pl.when(core == 1)
    def _():
        tell(known_sem.at[0], {"tp": 1 - core})

    replies = has_outward.astype(jnp.int32) + 2 - side - core

    @pl.when(replies > 0)
    def _():
        pl.semaphore_wait(known_sem.at[0], replies)

    tell_neighbours(known_sem.at[1])
    pl.semaphore_wait(known_sem.at[1], neighbours)
    tell_neighbours(known_sem.at[2])

    def query_copy(owner):
        return pltpu.make_async_remote_copy(
            src_ref=query_in.at[me], dst_ref=query_in.at[me],
            send_sem=query_sent.at[owner], recv_sem=query_recv.at[me],
            device_id={"sp": owner}, device_id_type=MESH,
        )

    def gate_copy(owner):
        return pltpu.make_async_remote_copy(
            src_ref=gate_send.at[owner], dst_ref=gate_in.at[me],
            send_sem=gate_sent.at[owner], recv_sem=gate_recv.at[me],
            device_id={"sp": owner}, device_id_type=MESH,
        )

    def part_copy(owner):
        return pltpu.make_async_remote_copy(
            src_ref=part_send.at[owner], dst_ref=part_in.at[me],
            send_sem=part_sent.at[owner], recv_sem=part_recv.at[me],
            device_id={"sp": owner}, device_id_type=MESH,
        )

    def block_copy(owner, t, size=tile):
        return pltpu.make_async_remote_copy(
            src_ref=outgoing.at[owner, :, pl.ds(t * tile, size), :],
            dst_ref=kv.at[:, pl.ds(pl.multiple_of(me * count + t * tile, LANES), size), :],
            send_sem=send_sem.at[owner, t], recv_sem=recv_sem.at[me, t],
            device_id={"sp": owner}, device_id_type=MESH,
        )

    def both_sizes(t, short, act):
        if t == ahead_tile:
            @pl.when(short)
            def _():
                act(tile - ahead_rows)

            @pl.when(jnp.logical_not(short))
            def _():
                act(tile)
        else:
            act(tile)

    def block_own(t):
        return pltpu.make_async_copy(
            outgoing.at[me, :, pl.ds(t * tile, tile), :],
            kv.at[:, pl.ds(pl.multiple_of(me * count + t * tile, tile), tile), :],
            recv_sem.at[me, t],
        )

    def send_block(owner, t):
        @pl.when(owner != me)
        def _():
            both_sizes(t, inner & crosses(owner), lambda size: block_copy(owner, t, size).start())

        @pl.when(owner == me)
        def _():
            block_own(t).start()

    def own_gates(owner, span):
        return jnp.concatenate([gate_own[owner, h, :, span] for h in range(per_owner)], axis=0)

    low = lax.broadcasted_iota(jnp.int32, (tile, LANES), 1) < head

    def open_links(first_round, last_round):
        for at in range(first_round - 1, last_round):
            pl.semaphore_wait(known_sem.at[at], neighbours)
            if at + 1 < layers:
                tell_neighbours(known_sem.at[at + 1])

    def send_queries():
        load_gates.wait()
        load_query.wait()
        wide = jnp.concatenate(
            [query_own[...].astype(jnp.float32), jnp.zeros((per_owner, LANES - head), jnp.float32)], axis=1
        ) * (head ** -0.5)
        query_in[me] = wide.astype(jnp.bfloat16)

        @pl.loop(0, n - 1)
        def _(k):
            query_copy(partner(k, me, n)).start()

    def send_gates():
        @pl.loop(0, n - 1)
        def _(k):
            owner = partner(k, me, n)
            gate_send[owner] = own_gates(owner, slice(None)).astype(jnp.bfloat16)
            gate_copy(owner).start()

        gate_in[me] = own_gates(me, slice(None)).astype(jnp.bfloat16)

    head_row = lax.broadcasted_iota(jnp.int32, (per_owner, LANES), 0)
    tile_row = lax.broadcasted_iota(jnp.int32, (per_owner, tile), 0)
    lane = lax.broadcasted_iota(jnp.int32, (per_owner, LANES), 1)

    def read_own(owner):
        @pl.when(owner != me)
        def _():
            pltpu.make_async_copy(query_in.at[owner], query_in.at[owner], query_recv.at[owner]).wait()

        asked = query_in[owner].astype(jnp.float32)
        queries = [
            jnp.where(head_row == h, asked, 0.0).astype(jnp.bfloat16) for h in range(per_owner)
        ]
        top = jnp.full((per_owner, 1), -1e30, jnp.float32)
        total = jnp.zeros((per_owner, 1), jnp.float32)
        weighted = jnp.zeros((per_owner, LANES), jnp.float32)
        for t in range(tiles):
            span = pl.ds(t * tile, tile)
            blocks = [outgoing[owner, h, span, :] for h in range(per_owner)]
            scores = None
            for h in range(per_owner):
                term = lax.dot_general(
                    queries[h], blocks[h], (((1,), (1,)), ((), ())), preferred_element_type=jnp.float32
                )
                scores = term if scores is None else scores + term
            scores = scores - own_gates(owner, span)
            new_top = jnp.maximum(top, jnp.max(scores, axis=1, keepdims=True))
            scale = jnp.exp(top - new_top)
            probs = jnp.exp(scores - new_top)
            total = total * scale + jnp.sum(probs, axis=1, keepdims=True)
            weighted = weighted * scale
            for h in range(per_owner):
                picked = jnp.where(tile_row == h, probs, 0.0).astype(jnp.bfloat16)
                weighted = weighted + jnp.dot(picked, blocks[h], preferred_element_type=jnp.float32)
            top = new_top
        packed = jnp.where(lane < head // 2, top, jnp.where(lane < head, total, weighted))
        part_send[owner] = packed

        @pl.when(owner != me)
        def _():
            part_copy(owner).start()

    def project(step, first, relays=False):
        group = group_of(step)

        if first:
            for ahead in range(1, min(3, groups)):
                load_weight(ahead, 0).start()
                load_weight(ahead, 1).start()
        else:
            @pl.when(step + 2 < groups)
            def _():
                load_weight(step + 2, 0).start()
                load_weight(step + 2, 1).start()

        load_weight(step, 0).wait()
        load_weight(step, 1).wait()

        def multiply(left, store):
            size = left.shape[0]
            keys = jnp.dot(left, weights[step, 0], preferred_element_type=jnp.float32)
            values = jnp.dot(left, weights[step, 1], preferred_element_type=jnp.float32)
            for pair in range(columns // LANES):
                span = slice(pair * LANES, (pair + 1) * LANES)
                k, v = keys[:, span], values[:, span]
                joined = (
                    jnp.where(low[:size], k, pltpu.roll(v, head, 1)),
                    jnp.where(low[:size], pltpu.roll(k, head, 1), v),
                )
                for half in range(2):
                    local = pair * 2 + half
                    store(
                        group * owners + local // per_owner, local % per_owner, joined[half].astype(jnp.bfloat16)
                    )

        for t in range(tiles):
            if first:
                load_rows(t).wait()

            def keep(owner, h, block):
                outgoing[owner, h, pl.ds(t * tile, tile), :] = block

            multiply(rows[pl.ds(t * tile, tile), :], keep)
            if first and t == 0:
                open_links(3, near + 1)

                @pl.when(inner)
                def _():
                    for j in range(owners):
                        send_block(group * owners + j, t)

                open_links(near + 2, layers)

                @pl.when(jnp.logical_not(inner))
                def _():
                    for j in range(owners):
                        send_block(group * owners + j, t)
            elif t < early:
                for j in range(owners):
                    send_block(group * owners + j, t)
            if first and t == 0:
                send_queries()
        for j in range(owners):
            read_own(group * owners + j)
        if relays:
            @pl.when(inner)
            def _():
                def keep(owner, h, block):
                    relayed[owner, h] = block

                multiply(row_in[...], keep)
                for j in range(owners):
                    owner = group * owners + j

                    @pl.when(owner != me)
                    def _():
                        relay_copy(owner).start()

                    @pl.when(owner == me)
                    def _():
                        kv[:, mate_rows, :] = relayed[owner]

    mate_rows = pl.ds(pl.multiple_of(mate * count + ahead_at, 16), ahead_rows)

    def relay_copy(owner):
        return pltpu.make_async_remote_copy(
            src_ref=relayed.at[owner], dst_ref=kv.at[:, mate_rows, :],
            send_sem=relay_sent.at[owner], recv_sem=relay_recv.at[me],
            device_id={"sp": owner}, device_id_type=MESH,
        )

    project(0, True)
    send_gates()

    def across(step, carry):
        project(step, False)
        return carry

    lax.fori_loop(1, groups // 2, across, 0)

    @pl.when(inner)
    def _():
        send_ahead.wait()

    def along(step, carry):
        project(step, False, True)
        return carry

    lax.fori_loop(groups // 2, groups, along, 0)

    if early < tiles:
        @pl.when(core == 0)
        def _():
            @pl.loop(0, n)
            def _(k):
                for t in range(early, tiles):
                    send_block(partner(k, me, n), t)

    @pl.loop(0, n - 1)
    def _(k):
        source = partner(k, me, n)
        gate_copy(source).wait_send()
        query_copy(source).wait_send()
        pltpu.make_async_copy(gate_in.at[source], gate_in.at[source], gate_recv.at[source]).wait()

    for source in range(n):
        gate_out[:, source * count:(source + 1) * count] = gate_in[source].astype(jnp.float32)

    def merge(one, two):
        top_one, top_two = one[:, :1], two[:, :1]
        joint = jnp.maximum(top_one, top_two)
        both = one * jnp.exp(top_one - joint) + two * jnp.exp(top_two - joint)
        return jnp.where(lane < head // 2, joint, both)

    def gather(k, carry):
        source = partner(n - 2 - k, me, n)
        part_copy(source).wait_send()
        pltpu.make_async_copy(part_in.at[source], part_in.at[source], part_recv.at[source]).wait()
        return merge(carry, part_in[source])

    packed = lax.fori_loop(0, n - 1, gather, part_send[me])
    mine[...] = packed
    swap = pltpu.make_async_remote_copy(
        src_ref=mine, dst_ref=theirs, send_sem=pair_sem.at[0], recv_sem=pair_sem.at[1],
        device_id={"tp": 1 - core}, device_id_type=MESH,
    )
    swap.start()
    swap.wait()
    other = theirs[...]
    joint = merge(jnp.where(core == 0, packed, other), jnp.where(core == 0, other, packed))
    at = head // 2
    answer = joint / joint[:, at:at + 1]
    read[...] = pltpu.roll(answer, head, 1)[:, :head].astype(jnp.bfloat16)

    def settle(t):
        block_own(t).wait()

        @pl.loop(0, n - 1)
        def _(k):
            source = partner(n - 2 - k, me, n)
            both_sizes(t, inner & crosses(source), lambda size: block_copy(source, t, size).wait_send())

            def arrived(size):
                span = pl.ds(t * tile, size)
                pltpu.make_async_copy(kv.at[:, span, :], kv.at[:, span, :], recv_sem.at[source, t]).wait()

            both_sizes(t, is_inner(source) & crosses(source), arrived)

    first_inner = jnp.where(right, near, near - 1) * 2

    @pl.loop(0, 2)
    def _(k):
        source = first_inner + k

        @pl.when(source != me)
        def _():
            pltpu.make_async_copy(
                kv.at[:, ahead_span, :], kv.at[:, ahead_span, :], relay_recv.at[source]
            ).wait()

    @pl.when(inner)
    def _():
        @pl.loop(0, n // 2)
        def _(k):
            owner = jnp.where(right, n // 2, 0) + k

            @pl.when(owner != me)
            def _():
                relay_copy(owner).wait_send()

    for t in range(early):
        settle(t)
    if early < tiles:
        @pl.when(core == 0)
        def _():
            for t in range(early, tiles):
                settle(t)


def rest_kernel(
    n, first_row,
    outgoing, after,
    late,
    send_sem, recv_sem,
):
    me = lax.axis_index("sp")
    size = outgoing.shape[2] - first_row
    held = pl.ds(first_row, size)

    def rows_of(source):
        return pl.ds(pl.multiple_of(source * size, size), size)

    def block_copy(owner):
        return pltpu.make_async_remote_copy(
            src_ref=outgoing.at[owner, :, held, :], dst_ref=late.at[:, rows_of(me), :],
            send_sem=send_sem.at[owner], recv_sem=recv_sem.at[me],
            device_id={"sp": owner}, device_id_type=MESH,
        )

    @pl.when(lax.axis_index("tp") == 1)
    def _():
        barrier = pltpu.get_barrier_semaphore()

        @pl.loop(1, n)
        def _(k):
            pl.semaphore_signal(
                barrier, inc=1, device_id={"sp": lax.rem(me + k, n)}, device_id_type=MESH
            )

        pl.semaphore_wait(barrier, n - 1)

        @pl.loop(0, n - 1)
        def _(k):
            block_copy(partner(k, me, n, 1)).start()

        late[:, rows_of(me), :] = outgoing[me, :, held, :]

        @pl.loop(0, n - 1)
        def _(k):
            source = partner(n - 2 - k, me, n)
            block_copy(source).wait_send()
            pltpu.make_async_copy(
                outgoing.at[0, :, held, :], late.at[:, rows_of(source), :], recv_sem.at[source]
            ).wait()


def finish_kernel(n, first_row, kv, gates, answer, kv_out, gate_out, read, after, sem):
    count = kv.shape[1] // n

    def part(source, start, size, at):
        span = pl.ds(source * count + start, size)
        return pltpu.make_async_copy(kv.at[:, span, :], kv_out.at[:, span, :], sem.at[at])

    small = [
        pltpu.make_async_copy(gates, gate_out, sem.at[2 * n]),
        pltpu.make_async_copy(answer, read, sem.at[2 * n + 1]),
    ]
    early = [part(source, 0, first_row, source) for source in range(n)]
    for copy in early + small:
        copy.start()
    after[...] = jnp.zeros_like(after)
    if first_row < count:
        @pl.when(lax.axis_index("tp") == 0)
        def _():
            late = [part(source, first_row, count - first_row, n + source) for source in range(n)]
            for copy in late:
                copy.start()
            for copy in late:
                copy.wait()
    for copy in early + small:
        copy.wait()


def last_kernel(n, first_row, late, kv, kv_out, sem):
    count = kv_out.shape[1] // n
    size = count - first_row

    @pl.when(lax.axis_index("tp") == 1)
    def _():
        copies = [
            pltpu.make_async_copy(
                late.at[:, pl.ds(source * size, size), :],
                kv_out.at[:, pl.ds(source * count + first_row, size), :],
                sem.at[source],
            )
            for source in range(n)
        ]
        for copy in copies:
            copy.start()
        for copy in copies:
            copy.wait()


def on_device(n, tokens, key_weight, value_weight, cum_gate, query):
    _, _, count, width = tokens.shape
    heads = cum_gate.shape[1]
    per_owner, head = query.shape[1], query.shape[2]
    tile = 256 if count % 256 == 0 else count
    columns = max(per_owner * head, LANES)
    groups = heads * head // columns
    tiles = count // tile
    ahead_rows = tile // 8
    any_space = pl.BlockSpec(memory_space=pl.ANY)
    outside = pl.BlockSpec(memory_space=pltpu.HBM)
    vmem = pl.BlockSpec(memory_space=pltpu.VMEM)
    kv, outgoing, gates, answer = pl.pallas_call(
        functools.partial(exchange_kernel, n, per_owner, tile, head, ahead_rows),
        name="exchange",
        out_shape=(
            pltpu.VMEM((per_owner, n * count, 2 * head), jnp.bfloat16),
            pltpu.VMEM((n, per_owner, count, 2 * head), jnp.bfloat16),
            pltpu.VMEM((per_owner, n * count), jnp.float32),
            pltpu.VMEM((per_owner, head), jnp.bfloat16),
        ),
        in_specs=[outside] * 5,
        out_specs=(vmem, vmem, vmem, vmem),
        scratch_shapes=[
            pltpu.VMEM((count, width), jnp.bfloat16),
            pltpu.VMEM((groups, 2, width, columns), jnp.bfloat16),
            pltpu.VMEM((n, per_owner, 1, count), jnp.float32),
            pltpu.VMEM((n, per_owner, count), jnp.bfloat16),
            pltpu.VMEM((n, per_owner, count), jnp.bfloat16),
            pltpu.VMEM((per_owner, head), jnp.bfloat16),
            pltpu.VMEM((n, per_owner, LANES), jnp.bfloat16),
            pltpu.VMEM((n, per_owner, LANES), jnp.float32),
            pltpu.VMEM((n, per_owner, LANES), jnp.float32),
            pltpu.VMEM((per_owner, LANES), jnp.float32),
            pltpu.VMEM((per_owner, LANES), jnp.float32),
            pltpu.VMEM((ahead_rows, width), jnp.bfloat16),
            pltpu.VMEM((n, per_owner, ahead_rows, 2 * head), jnp.bfloat16),
            pltpu.SemaphoreType.DMA((tiles,)),
            pltpu.SemaphoreType.DMA((groups, 2)),
            pltpu.SemaphoreType.DMA((3,)),
            pltpu.SemaphoreType.DMA((n, tiles)),
            pltpu.SemaphoreType.DMA((n, tiles)),
            pltpu.SemaphoreType.REGULAR((n // 2,)),
            pltpu.SemaphoreType.DMA((2,)),
            pltpu.SemaphoreType.DMA((n,)),
            pltpu.SemaphoreType.DMA((n,)),
            pltpu.SemaphoreType.DMA((n,)),
            pltpu.SemaphoreType.DMA((n,)),
            pltpu.SemaphoreType.DMA((n,)),
            pltpu.SemaphoreType.DMA((n,)),
            pltpu.SemaphoreType.DMA((n,)),
            pltpu.SemaphoreType.DMA((n,)),
            pltpu.SemaphoreType.DMA((2,)),
        ],
        compiler_params=pltpu.CompilerParams(
            collective_id=0, has_side_effects=True, vmem_limit_bytes=48 * 1024 * 1024
        ),
    )(
        tokens.reshape(count, width),
        key_weight,
        value_weight,
        cum_gate.reshape(n, per_owner, 1, count),
        query.reshape(per_owner, head),
    )
    first_row = max(tiles - 1, 1) * tile
    whole = jax.ShapeDtypeStruct((per_owner, n * count, 2 * head), jnp.bfloat16)
    kv_out, gate_out, read, after = pl.pallas_call(
        functools.partial(finish_kernel, n, first_row),
        name="finish",
        out_shape=(
            whole,
            jax.ShapeDtypeStruct((per_owner, n * count), jnp.float32),
            jax.ShapeDtypeStruct((per_owner, head), jnp.bfloat16),
            pltpu.VMEM((8, LANES), jnp.float32),
        ),
        in_specs=[vmem, vmem, vmem],
        out_specs=(any_space, any_space, any_space, vmem),
        scratch_shapes=[pltpu.SemaphoreType.DMA((2 * n + 2,))],
        compiler_params=pltpu.CompilerParams(vmem_limit_bytes=16 * 1024 * 1024),
    )(kv, gates, answer)
    if first_row < count:
        late = pl.pallas_call(
            functools.partial(rest_kernel, n, first_row),
            name="rest",
            out_shape=pltpu.VMEM((per_owner, n * (count - first_row), 2 * head), jnp.bfloat16),
            in_specs=[vmem, vmem],
            out_specs=vmem,
            scratch_shapes=[pltpu.SemaphoreType.DMA((n,)), pltpu.SemaphoreType.DMA((n,))],
            compiler_params=pltpu.CompilerParams(
                collective_id=1, has_side_effects=True, vmem_limit_bytes=16 * 1024 * 1024
            ),
        )(outgoing, after)
        kv_out = pl.pallas_call(
            functools.partial(last_kernel, n, first_row),
            name="last",
            out_shape=whole,
            in_specs=[vmem, any_space],
            out_specs=any_space,
            input_output_aliases={1: 0},
            scratch_shapes=[pltpu.SemaphoreType.DMA((n,))],
            compiler_params=pltpu.CompilerParams(vmem_limit_bytes=16 * 1024 * 1024),
        )(late, kv_out)
    return kv_out[None], gate_out[None], read[None]


def solution(mesh):
    placed = (P("gr", "tp", "sp", None), P(), P(), P("gr", None, "tp", "sp"), P("gr", "sp", None))
    return jax.shard_map(
        functools.partial(on_device, mesh.shape["sp"]),
        mesh=mesh,
        in_specs=placed,
        out_specs=(P("gr", "sp", "tp", None), P("gr", "sp", "tp"), P("gr", "sp", None)),
        check_vma=False,
    )
```

```python
import functools

import jax
import jax.numpy as jnp
from jax import lax
from jax.experimental import pallas as pl
from jax.experimental.pallas import tpu as pltpu
from jax.sharding import PartitionSpec as P

MESH = pl.DeviceIdType.MESH
LANES = 128


def partner(step, me, n, turned=0):
    turn, flip = step // 2, lax.rem(step + turned, 2)
    flip = jnp.where(turn == n // 2 - 1, 1 - lax.rem(step, 2), flip)
    half = n // 4
    at = me // 2
    far = at >= half
    w = jnp.where(far, 2 * half - 1 - at, at)
    goal = jnp.where(turn < half, 2 * half - 1 - turn, lax.rem(w + 1 + turn, half))
    goal = jnp.where(far, 2 * half - 1 - goal, goal)
    return goal * 2 + lax.rem(me + flip, 2)


def exchange_kernel(
    n, per_owner, tile, head, ahead_rows,
    tokens, key_weight, value_weight, gates, query,
    kv, outgoing, gate_out, read,
    rows, weights, gate_own, gate_send, gate_in, query_own, query_in, part_send, part_in, mine, theirs, row_in, relayed,
    row_sem, weight_sem, small_sem, send_sem, recv_sem, known_sem, ahead_sem, relay_sent, relay_recv,
    gate_sent, gate_recv, query_sent, query_recv, part_sent, part_recv, pair_sem,
):
    me = lax.axis_index("sp")
    core = lax.axis_index("tp")
    count = rows.shape[0]
    tiles = count // tile
    early = max(tiles - 1, 1)
    columns = weights.shape[3]
    group_heads = columns // head
    owners = group_heads // per_owner
    groups = n // owners

    def group_of(step):
        return partner(step, me // owners, groups, core)

    def load_rows(t):
        span = pl.ds(t * tile, tile - ahead_rows if t == early - 1 else tile)
        return pltpu.make_async_copy(tokens.at[span, :], rows.at[span, :], row_sem.at[t])

    def load_weight(step, which):
        at = pl.ds(pl.multiple_of(group_of(step) * columns, columns), columns)
        source = (key_weight, value_weight)[which]
        return pltpu.make_async_copy(
            source.at[:, at], weights.at[step, which], weight_sem.at[step, which]
        )

    load_query = pltpu.make_async_copy(query, query_own, small_sem.at[0])
    load_gates = pltpu.make_async_copy(gates, gate_own, small_sem.at[1])

    layers = n // 2
    layer = me // 2
    near = layers // 2
    right = layer >= near
    inner = (layer == near - 1) | (layer == near)
    mate = jnp.where(right, me - 2, me + 2)
    ahead_tile = early - 1
    ahead_at = (ahead_tile + 1) * tile - ahead_rows
    ahead_span = pl.ds(ahead_at, ahead_rows)

    def crosses(owner):
        return (owner // 2 >= near) != right

    def is_inner(owner):
        return (owner // 2 == near - 1) | (owner // 2 == near)

    barrier = pltpu.get_barrier_semaphore()
    neighbours = 1 + (layer > 0).astype(jnp.int32) + (layer < layers - 1).astype(jnp.int32)

    def tell_neighbours(sem):
        @pl.when(layer > 0)
        def _():
            pl.semaphore_signal(sem, inc=1, device_id={"sp": me - 2}, device_id_type=MESH)

        @pl.when(layer < layers - 1)
        def _():
            pl.semaphore_signal(sem, inc=1, device_id={"sp": me + 2}, device_id_type=MESH)

        pl.semaphore_signal(
            sem, inc=1, device_id={"sp": me + 1 - 2 * lax.rem(me, 2)}, device_id_type=MESH
        )

    side = lax.rem(me, 2)
    outward = jnp.where(right, me + 2, me - 2)
    inward = jnp.where(right, me - 2, me + 2)
    has_outward = jnp.logical_not((layer == 0) | (layer == layers - 1))

    def tell(sem, to):
        pl.semaphore_signal(sem, inc=1, device_id=to, device_id_type=MESH)

    @pl.when(inner)
    def _():
        tell(barrier, {"sp": mate})

    @pl.when(side == 0)
    def _():
        tell(barrier, {"sp": me + 1})

    @pl.when(core == 0)
    def _():
        tell(barrier, {"tp": 1 - core})

    @pl.when(has_outward)
    def _():
        tell(barrier, {"sp": outward})

    load_ahead = pltpu.make_async_copy(
        tokens.at[ahead_span, :], rows.at[ahead_span, :], small_sem.at[2]
    )
    load_ahead.start()
    load_rows(0).start()
    load_weight(0, 0).start()
    load_weight(0, 1).start()
    load_gates.start()
    load_query.start()
    for t in range(1, tiles):
        load_rows(t).start()
    send_ahead = pltpu.make_async_remote_copy(
        src_ref=rows.at[ahead_span, :], dst_ref=row_in,
        send_sem=ahead_sem.at[0], recv_sem=ahead_sem.at[1],
        device_id={"sp": mate}, device_id_type=MESH,
    )
    load_ahead.wait()
    pl.semaphore_wait(barrier, 1 + side + core)

    @pl.when(inner)
    def _():
        send_ahead.start()

    @pl.when(jnp.logical_not(inner))
    def _():
        tell(known_sem.at[0], {"sp": inward})

    @pl.when(side == 1)
    def _():
        tell(known_sem.at[0], {"sp": me - 1})

    @pl.when(core == 1)
    def _():
        tell(known_sem.at[0], {"tp": 1 - core})

    replies = has_outward.astype(jnp.int32) + 2 - side - core

    @pl.when(replies > 0)
    def _():
        pl.semaphore_wait(known_sem.at[0], replies)

    tell_neighbours(known_sem.at[1])
    pl.semaphore_wait(known_sem.at[1], neighbours)
    tell_neighbours(known_sem.at[2])

    def query_copy(owner):
        return pltpu.make_async_remote_copy(
            src_ref=query_in.at[me], dst_ref=query_in.at[me],
            send_sem=query_sent.at[owner], recv_sem=query_recv.at[me],
            device_id={"sp": owner}, device_id_type=MESH,
        )

    def gate_copy(owner):
        return pltpu.make_async_remote_copy(
            src_ref=gate_send.at[owner], dst_ref=gate_in.at[me],
            send_sem=gate_sent.at[owner], recv_sem=gate_recv.at[me],
            device_id={"sp": owner}, device_id_type=MESH,
        )

    def part_copy(owner):
        return pltpu.make_async_remote_copy(
            src_ref=part_send.at[owner], dst_ref=part_in.at[me],
            send_sem=part_sent.at[owner], recv_sem=part_recv.at[me],
            device_id={"sp": owner}, device_id_type=MESH,
        )

    def block_copy(owner, t, size=tile):
        return pltpu.make_async_remote_copy(
            src_ref=outgoing.at[owner, :, pl.ds(t * tile, size), :],
            dst_ref=kv.at[:, pl.ds(pl.multiple_of(me * count + t * tile, LANES), size), :],
            send_sem=send_sem.at[owner, t], recv_sem=recv_sem.at[me, t],
            device_id={"sp": owner}, device_id_type=MESH,
        )

    def both_sizes(t, short, act):
        if t == ahead_tile:
            @pl.when(short)
            def _():
                act(tile - ahead_rows)

            @pl.when(jnp.logical_not(short))
            def _():
                act(tile)
        else:
            act(tile)

    def block_own(t):
        return pltpu.make_async_copy(
            outgoing.at[me, :, pl.ds(t * tile, tile), :],
            kv.at[:, pl.ds(pl.multiple_of(me * count + t * tile, tile), tile), :],
            recv_sem.at[me, t],
        )

    def send_block(owner, t):
        @pl.when(owner != me)
        def _():
            both_sizes(t, inner & crosses(owner), lambda size: block_copy(owner, t, size).start())

        @pl.when(owner == me)
        def _():
            block_own(t).start()

    def own_gates(owner, span):
        return jnp.concatenate([gate_own[owner, h, :, span] for h in range(per_owner)], axis=0)

    low = lax.broadcasted_iota(jnp.int32, (tile, LANES), 1) < head

    def open_links(first_round, last_round):
        for at in range(first_round - 1, last_round):
            pl.semaphore_wait(known_sem.at[at], neighbours)
            if at + 1 < layers:
                tell_neighbours(known_sem.at[at + 1])

    def send_queries():
        load_gates.wait()
        load_query.wait()
        wide = jnp.concatenate(
            [query_own[...].astype(jnp.float32), jnp.zeros((per_owner, LANES - head), jnp.float32)], axis=1
        ) * (head ** -0.5)
        query_in[me] = wide.astype(jnp.bfloat16)

        @pl.loop(0, n - 1)
        def _(k):
            query_copy(partner(k, me, n)).start()

    def send_gates():
        @pl.loop(0, n - 1)
        def _(k):
            owner = partner(k, me, n)
            gate_send[owner] = own_gates(owner, slice(None)).astype(jnp.bfloat16)
            gate_copy(owner).start()

        gate_in[me] = own_gates(me, slice(None)).astype(jnp.bfloat16)

    head_row = lax.broadcasted_iota(jnp.int32, (per_owner, LANES), 0)
    tile_row = lax.broadcasted_iota(jnp.int32, (per_owner, tile), 0)
    lane = lax.broadcasted_iota(jnp.int32, (per_owner, LANES), 1)

    def read_own(owner):
        @pl.when(owner != me)
        def _():
            pltpu.make_async_copy(query_in.at[owner], query_in.at[owner], query_recv.at[owner]).wait()

        asked = query_in[owner].astype(jnp.float32)
        queries = [
            jnp.where(head_row == h, asked, 0.0).astype(jnp.bfloat16) for h in range(per_owner)
        ]
        top = jnp.full((per_owner, 1), -1e30, jnp.float32)
        total = jnp.zeros((per_owner, 1), jnp.float32)
        weighted = jnp.zeros((per_owner, LANES), jnp.float32)
        for t in range(tiles):
            span = pl.ds(t * tile, tile)
            blocks = [outgoing[owner, h, span, :] for h in range(per_owner)]
            scores = None
            for h in range(per_owner):
                term = lax.dot_general(
                    queries[h], blocks[h], (((1,), (1,)), ((), ())), preferred_element_type=jnp.float32
                )
                scores = term if scores is None else scores + term
            scores = scores - own_gates(owner, span)
            new_top = jnp.maximum(top, jnp.max(scores, axis=1, keepdims=True))
            scale = jnp.exp(top - new_top)
            probs = jnp.exp(scores - new_top)
            total = total * scale + jnp.sum(probs, axis=1, keepdims=True)
            weighted = weighted * scale
            for h in range(per_owner):
                picked = jnp.where(tile_row == h, probs, 0.0).astype(jnp.bfloat16)
                weighted = weighted + jnp.dot(picked, blocks[h], preferred_element_type=jnp.float32)
            top = new_top
        level = top + jnp.log(total)
        first = level.astype(jnp.bfloat16).astype(jnp.float32)
        second = (level - first).astype(jnp.bfloat16).astype(jnp.float32)
        third = level - first - second
        words = jnp.where(lane == 0, first, jnp.where(lane == 1, second, third))
        part_send[owner] = jnp.where(lane < head, words, weighted / total).astype(jnp.bfloat16)

        @pl.when(owner != me)
        def _():
            part_copy(owner).start()

    def project(step, first, relays=False):
        group = group_of(step)

        if first:
            for ahead in range(1, min(3, groups)):
                load_weight(ahead, 0).start()
                load_weight(ahead, 1).start()
        else:
            @pl.when(step + 2 < groups)
            def _():
                load_weight(step + 2, 0).start()
                load_weight(step + 2, 1).start()

        load_weight(step, 0).wait()
        load_weight(step, 1).wait()

        def multiply(left, store):
            size = left.shape[0]
            keys = jnp.dot(left, weights[step, 0], preferred_element_type=jnp.float32)
            values = jnp.dot(left, weights[step, 1], preferred_element_type=jnp.float32)
            for pair in range(columns // LANES):
                span = slice(pair * LANES, (pair + 1) * LANES)
                k, v = keys[:, span], values[:, span]
                joined = (
                    jnp.where(low[:size], k, pltpu.roll(v, head, 1)),
                    jnp.where(low[:size], pltpu.roll(k, head, 1), v),
                )
                for half in range(2):
                    local = pair * 2 + half
                    store(
                        group * owners + local // per_owner, local % per_owner, joined[half].astype(jnp.bfloat16)
                    )

        for t in range(tiles):
            if first:
                load_rows(t).wait()

            def keep(owner, h, block):
                outgoing[owner, h, pl.ds(t * tile, tile), :] = block

            multiply(rows[pl.ds(t * tile, tile), :], keep)
            if first and t == 0:
                open_links(3, near + 1)

                @pl.when(inner)
                def _():
                    for j in range(owners):
                        send_block(group * owners + j, t)

                open_links(near + 2, layers)

                @pl.when(jnp.logical_not(inner))
                def _():
                    for j in range(owners):
                        send_block(group * owners + j, t)
            elif t < early:
                for j in range(owners):
                    send_block(group * owners + j, t)
            if first and t == 0:
                send_queries()
        for j in range(owners):
            read_own(group * owners + j)
        if relays:
            @pl.when(inner)
            def _():
                def keep(owner, h, block):
                    relayed[owner, h] = block

                multiply(row_in[...], keep)
                for j in range(owners):
                    owner = group * owners + j

                    @pl.when(owner != me)
                    def _():
                        relay_copy(owner).start()

                    @pl.when(owner == me)
                    def _():
                        kv[:, mate_rows, :] = relayed[owner]

    mate_rows = pl.ds(pl.multiple_of(mate * count + ahead_at, 16), ahead_rows)

    def relay_copy(owner):
        return pltpu.make_async_remote_copy(
            src_ref=relayed.at[owner], dst_ref=kv.at[:, mate_rows, :],
            send_sem=relay_sent.at[owner], recv_sem=relay_recv.at[me],
            device_id={"sp": owner}, device_id_type=MESH,
        )

    project(0, True)
    send_gates()

    def across(step, carry):
        project(step, False)
        return carry

    lax.fori_loop(1, groups // 2, across, 0)

    @pl.when(inner)
    def _():
        send_ahead.wait()

    def along(step, carry):
        project(step, False, True)
        return carry

    lax.fori_loop(groups // 2, groups, along, 0)

    if early < tiles:
        @pl.when(core == 0)
        def _():
            @pl.loop(0, n)
            def _(k):
                for t in range(early, tiles):
                    send_block(partner(k, me, n), t)

    @pl.loop(0, n - 1)
    def _(k):
        source = partner(k, me, n)
        gate_copy(source).wait_send()
        query_copy(source).wait_send()
        pltpu.make_async_copy(gate_in.at[source], gate_in.at[source], gate_recv.at[source]).wait()

    for source in range(n):
        gate_out[:, source * count:(source + 1) * count] = gate_in[source].astype(jnp.float32)

    def merge(one, two):
        top_one, top_two = one[:, :1], two[:, :1]
        joint = jnp.maximum(top_one, top_two)
        both = one * jnp.exp(top_one - joint) + two * jnp.exp(top_two - joint)
        return jnp.where(lane < head // 2, joint, both)

    def unpack(part):
        words = part.astype(jnp.float32)
        level = words[:, 0:1] + words[:, 1:2] + words[:, 2:3]
        return jnp.where(lane < head // 2, level, jnp.where(lane < head, 1.0, words))

    def gather(k, carry):
        source = partner(n - 2 - k, me, n)
        part_copy(source).wait_send()
        pltpu.make_async_copy(part_in.at[source], part_in.at[source], part_recv.at[source]).wait()
        return merge(carry, unpack(part_in[source]))

    packed = lax.fori_loop(0, n - 1, gather, unpack(part_send[me]))
    mine[...] = packed
    swap = pltpu.make_async_remote_copy(
        src_ref=mine, dst_ref=theirs, send_sem=pair_sem.at[0], recv_sem=pair_sem.at[1],
        device_id={"tp": 1 - core}, device_id_type=MESH,
    )
    swap.start()
    swap.wait()
    other = theirs[...]
    joint = merge(jnp.where(core == 0, packed, other), jnp.where(core == 0, other, packed))
    at = head // 2
    answer = joint / joint[:, at:at + 1]
    read[...] = pltpu.roll(answer, head, 1)[:, :head].astype(jnp.bfloat16)

    def settle(t):
        block_own(t).wait()

        @pl.loop(0, n - 1)
        def _(k):
            source = partner(n - 2 - k, me, n)
            both_sizes(t, inner & crosses(source), lambda size: block_copy(source, t, size).wait_send())

            def arrived(size):
                span = pl.ds(t * tile, size)
                pltpu.make_async_copy(kv.at[:, span, :], kv.at[:, span, :], recv_sem.at[source, t]).wait()

            both_sizes(t, is_inner(source) & crosses(source), arrived)

    first_inner = jnp.where(right, near, near - 1) * 2

    @pl.loop(0, 2)
    def _(k):
        source = first_inner + k

        @pl.when(source != me)
        def _():
            pltpu.make_async_copy(
                kv.at[:, ahead_span, :], kv.at[:, ahead_span, :], relay_recv.at[source]
            ).wait()

    @pl.when(inner)
    def _():
        @pl.loop(0, n // 2)
        def _(k):
            owner = jnp.where(right, n // 2, 0) + k

            @pl.when(owner != me)
            def _():
                relay_copy(owner).wait_send()

    for t in range(early):
        settle(t)
    if early < tiles:
        @pl.when(core == 0)
        def _():
            for t in range(early, tiles):
                settle(t)


def rest_kernel(
    n, first_row,
    outgoing, after,
    late,
    send_sem, recv_sem,
):
    me = lax.axis_index("sp")
    size = outgoing.shape[2] - first_row
    held = pl.ds(first_row, size)

    def rows_of(source):
        return pl.ds(pl.multiple_of(source * size, size), size)

    def block_copy(owner):
        return pltpu.make_async_remote_copy(
            src_ref=outgoing.at[owner, :, held, :], dst_ref=late.at[:, rows_of(me), :],
            send_sem=send_sem.at[owner], recv_sem=recv_sem.at[me],
            device_id={"sp": owner}, device_id_type=MESH,
        )

    @pl.when(lax.axis_index("tp") == 1)
    def _():
        barrier = pltpu.get_barrier_semaphore()

        @pl.loop(1, n)
        def _(k):
            pl.semaphore_signal(
                barrier, inc=1, device_id={"sp": lax.rem(me + k, n)}, device_id_type=MESH
            )

        pl.semaphore_wait(barrier, n - 1)

        @pl.loop(0, n - 1)
        def _(k):
            block_copy(partner(k, me, n, 1)).start()

        late[:, rows_of(me), :] = outgoing[me, :, held, :]

        @pl.loop(0, n - 1)
        def _(k):
            source = partner(n - 2 - k, me, n)
            block_copy(source).wait_send()
            pltpu.make_async_copy(
                outgoing.at[0, :, held, :], late.at[:, rows_of(source), :], recv_sem.at[source]
            ).wait()


def finish_kernel(n, first_row, kv, gates, answer, kv_out, gate_out, read, after, sem):
    count = kv.shape[1] // n

    def part(source, start, size, at):
        span = pl.ds(source * count + start, size)
        return pltpu.make_async_copy(kv.at[:, span, :], kv_out.at[:, span, :], sem.at[at])

    small = [
        pltpu.make_async_copy(gates, gate_out, sem.at[2 * n]),
        pltpu.make_async_copy(answer, read, sem.at[2 * n + 1]),
    ]
    early = [part(source, 0, first_row, source) for source in range(n)]
    for copy in early + small:
        copy.start()
    after[...] = jnp.zeros_like(after)
    if first_row < count:
        @pl.when(lax.axis_index("tp") == 0)
        def _():
            late = [part(source, first_row, count - first_row, n + source) for source in range(n)]
            for copy in late:
                copy.start()
            for copy in late:
                copy.wait()
    for copy in early + small:
        copy.wait()


def last_kernel(n, first_row, late, kv, kv_out, sem):
    count = kv_out.shape[1] // n
    size = count - first_row

    @pl.when(lax.axis_index("tp") == 1)
    def _():
        copies = [
            pltpu.make_async_copy(
                late.at[:, pl.ds(source * size, size), :],
                kv_out.at[:, pl.ds(source * count + first_row, size), :],
                sem.at[source],
            )
            for source in range(n)
        ]
        for copy in copies:
            copy.start()
        for copy in copies:
            copy.wait()


def on_device(n, tokens, key_weight, value_weight, cum_gate, query):
    _, _, count, width = tokens.shape
    heads = cum_gate.shape[1]
    per_owner, head = query.shape[1], query.shape[2]
    tile = 256 if count % 256 == 0 else count
    columns = max(per_owner * head, LANES)
    groups = heads * head // columns
    tiles = count // tile
    ahead_rows = tile // 8
    any_space = pl.BlockSpec(memory_space=pl.ANY)
    outside = pl.BlockSpec(memory_space=pltpu.HBM)
    vmem = pl.BlockSpec(memory_space=pltpu.VMEM)
    kv, outgoing, gates, answer = pl.pallas_call(
        functools.partial(exchange_kernel, n, per_owner, tile, head, ahead_rows),
        name="exchange",
        out_shape=(
            pltpu.VMEM((per_owner, n * count, 2 * head), jnp.bfloat16),
            pltpu.VMEM((n, per_owner, count, 2 * head), jnp.bfloat16),
            pltpu.VMEM((per_owner, n * count), jnp.float32),
            pltpu.VMEM((per_owner, head), jnp.bfloat16),
        ),
        in_specs=[outside] * 5,
        out_specs=(vmem, vmem, vmem, vmem),
        scratch_shapes=[
            pltpu.VMEM((count, width), jnp.bfloat16),
            pltpu.VMEM((groups, 2, width, columns), jnp.bfloat16),
            pltpu.VMEM((n, per_owner, 1, count), jnp.float32),
            pltpu.VMEM((n, per_owner, count), jnp.bfloat16),
            pltpu.VMEM((n, per_owner, count), jnp.bfloat16),
            pltpu.VMEM((per_owner, head), jnp.bfloat16),
            pltpu.VMEM((n, per_owner, LANES), jnp.bfloat16),
            pltpu.VMEM((n, per_owner, LANES), jnp.bfloat16),
            pltpu.VMEM((n, per_owner, LANES), jnp.bfloat16),
            pltpu.VMEM((per_owner, LANES), jnp.float32),
            pltpu.VMEM((per_owner, LANES), jnp.float32),
            pltpu.VMEM((ahead_rows, width), jnp.bfloat16),
            pltpu.VMEM((n, per_owner, ahead_rows, 2 * head), jnp.bfloat16),
            pltpu.SemaphoreType.DMA((tiles,)),
            pltpu.SemaphoreType.DMA((groups, 2)),
            pltpu.SemaphoreType.DMA((3,)),
            pltpu.SemaphoreType.DMA((n, tiles)),
            pltpu.SemaphoreType.DMA((n, tiles)),
            pltpu.SemaphoreType.REGULAR((n // 2,)),
            pltpu.SemaphoreType.DMA((2,)),
            pltpu.SemaphoreType.DMA((n,)),
            pltpu.SemaphoreType.DMA((n,)),
            pltpu.SemaphoreType.DMA((n,)),
            pltpu.SemaphoreType.DMA((n,)),
            pltpu.SemaphoreType.DMA((n,)),
            pltpu.SemaphoreType.DMA((n,)),
            pltpu.SemaphoreType.DMA((n,)),
            pltpu.SemaphoreType.DMA((n,)),
            pltpu.SemaphoreType.DMA((2,)),
        ],
        compiler_params=pltpu.CompilerParams(
            collective_id=0, has_side_effects=True, vmem_limit_bytes=48 * 1024 * 1024
        ),
    )(
        tokens.reshape(count, width),
        key_weight,
        value_weight,
        cum_gate.reshape(n, per_owner, 1, count),
        query.reshape(per_owner, head),
    )
    first_row = max(tiles - 1, 1) * tile
    whole = jax.ShapeDtypeStruct((per_owner, n * count, 2 * head), jnp.bfloat16)
    kv_out, gate_out, read, after = pl.pallas_call(
        functools.partial(finish_kernel, n, first_row),
        name="finish",
        out_shape=(
            whole,
            jax.ShapeDtypeStruct((per_owner, n * count), jnp.float32),
            jax.ShapeDtypeStruct((per_owner, head), jnp.bfloat16),
            pltpu.VMEM((8, LANES), jnp.float32),
        ),
        in_specs=[vmem, vmem, vmem],
        out_specs=(any_space, any_space, any_space, vmem),
        scratch_shapes=[pltpu.SemaphoreType.DMA((2 * n + 2,))],
        compiler_params=pltpu.CompilerParams(vmem_limit_bytes=16 * 1024 * 1024),
    )(kv, gates, answer)
    if first_row < count:
        late = pl.pallas_call(
            functools.partial(rest_kernel, n, first_row),
            name="rest",
            out_shape=pltpu.VMEM((per_owner, n * (count - first_row), 2 * head), jnp.bfloat16),
            in_specs=[vmem, vmem],
            out_specs=vmem,
            scratch_shapes=[pltpu.SemaphoreType.DMA((n,)), pltpu.SemaphoreType.DMA((n,))],
            compiler_params=pltpu.CompilerParams(
                collective_id=1, has_side_effects=True, vmem_limit_bytes=16 * 1024 * 1024
            ),
        )(outgoing, after)
        kv_out = pl.pallas_call(
            functools.partial(last_kernel, n, first_row),
            name="last",
            out_shape=whole,
            in_specs=[vmem, any_space],
            out_specs=any_space,
            input_output_aliases={1: 0},
            scratch_shapes=[pltpu.SemaphoreType.DMA((n,))],
            compiler_params=pltpu.CompilerParams(vmem_limit_bytes=16 * 1024 * 1024),
        )(late, kv_out)
    return kv_out[None], gate_out[None], read[None]


def solution(mesh):
    placed = (P("gr", "tp", "sp", None), P(), P(), P("gr", None, "tp", "sp"), P("gr", "sp", None))
    return jax.shard_map(
        functools.partial(on_device, mesh.shape["sp"]),
        mesh=mesh,
        in_specs=placed,
        out_specs=(P("gr", "sp", "tp", None), P("gr", "sp", "tp"), P("gr", "sp", None)),
        check_vma=False,
    )
```

```python
import functools

import jax
import jax.numpy as jnp
from jax import lax
from jax.experimental import pallas as pl
from jax.experimental.pallas import tpu as pltpu
from jax.sharding import PartitionSpec as P

MESH = pl.DeviceIdType.MESH
LANES = 128


def partner(step, me, n, turned=0):
    turn, flip = step // 2, lax.rem(step + turned, 2)
    flip = jnp.where(turn == n // 2 - 1, 1 - lax.rem(step, 2), flip)
    half = n // 4
    at = me // 2
    far = at >= half
    w = jnp.where(far, 2 * half - 1 - at, at)
    goal = jnp.where(turn < half, 2 * half - 1 - turn, lax.rem(w + 1 + turn, half))
    goal = jnp.where(far, 2 * half - 1 - goal, goal)
    return goal * 2 + lax.rem(me + flip, 2)


def exchange_kernel(
    n, per_owner, tile, head, ahead_rows,
    tokens, key_weight, value_weight, gates, query,
    kv, outgoing, gate_out, read,
    rows, weights, gate_own, gate_send, gate_in, query_own, query_in, part_send, part_in, mine, theirs, row_in, relayed,
    row_sem, weight_sem, small_sem, send_sem, recv_sem, known_sem, ahead_sem, relay_sent, relay_recv,
    gate_sent, gate_recv, query_sent, query_recv, part_sent, part_recv, pair_sem,
):
    me = lax.axis_index("sp")
    core = lax.axis_index("tp")
    count = rows.shape[0]
    tiles = count // tile
    early = max(tiles - 1, 1)
    columns = weights.shape[3]
    group_heads = columns // head
    owners = group_heads // per_owner
    groups = n // owners

    def group_of(step):
        return partner(step, me // owners, groups, core)

    def load_rows(t):
        span = pl.ds(t * tile, tile - ahead_rows if t == early - 1 else tile)
        return pltpu.make_async_copy(tokens.at[span, :], rows.at[span, :], row_sem.at[t])

    def load_weight(step, which):
        at = pl.ds(pl.multiple_of(group_of(step) * columns, columns), columns)
        source = (key_weight, value_weight)[which]
        return pltpu.make_async_copy(
            source.at[:, at], weights.at[step, which], weight_sem.at[step, which]
        )

    load_query = pltpu.make_async_copy(query, query_own, small_sem.at[0])
    load_gates = pltpu.make_async_copy(gates, gate_own, small_sem.at[1])

    layers = n // 2
    layer = me // 2
    near = layers // 2
    right = layer >= near
    inner = (layer == near - 1) | (layer == near)
    mate = jnp.where(right, me - 2, me + 2)
    ahead_tile = early - 1
    ahead_at = (ahead_tile + 1) * tile - ahead_rows
    ahead_span = pl.ds(ahead_at, ahead_rows)

    def crosses(owner):
        return (owner // 2 >= near) != right

    def is_inner(owner):
        return (owner // 2 == near - 1) | (owner // 2 == near)

    barrier = pltpu.get_barrier_semaphore()
    neighbours = 1 + (layer > 0).astype(jnp.int32) + (layer < layers - 1).astype(jnp.int32)

    def tell_neighbours(sem):
        @pl.when(layer > 0)
        def _():
            pl.semaphore_signal(sem, inc=1, device_id={"sp": me - 2}, device_id_type=MESH)

        @pl.when(layer < layers - 1)
        def _():
            pl.semaphore_signal(sem, inc=1, device_id={"sp": me + 2}, device_id_type=MESH)

        pl.semaphore_signal(
            sem, inc=1, device_id={"sp": me + 1 - 2 * lax.rem(me, 2)}, device_id_type=MESH
        )

    side = lax.rem(me, 2)
    outward = jnp.where(right, me + 2, me - 2)
    inward = jnp.where(right, me - 2, me + 2)
    has_outward = jnp.logical_not((layer == 0) | (layer == layers - 1))

    def tell(sem, to):
        pl.semaphore_signal(sem, inc=1, device_id=to, device_id_type=MESH)

    @pl.when(inner)
    def _():
        tell(barrier, {"sp": mate})

    @pl.when(side == 0)
    def _():
        tell(barrier, {"sp": me + 1})

    @pl.when(core == 0)
    def _():
        tell(barrier, {"tp": 1 - core})

    @pl.when(has_outward)
    def _():
        tell(barrier, {"sp": outward})

    load_ahead = pltpu.make_async_copy(
        tokens.at[ahead_span, :], rows.at[ahead_span, :], small_sem.at[2]
    )
    load_ahead.start()
    load_rows(0).start()
    load_weight(0, 0).start()
    load_weight(0, 1).start()
    load_gates.start()
    load_query.start()
    for t in range(1, tiles):
        load_rows(t).start()
    send_ahead = pltpu.make_async_remote_copy(
        src_ref=rows.at[ahead_span, :], dst_ref=row_in,
        send_sem=ahead_sem.at[0], recv_sem=ahead_sem.at[1],
        device_id={"sp": mate}, device_id_type=MESH,
    )
    load_ahead.wait()
    pl.semaphore_wait(barrier, 1 + side + core)

    @pl.when(inner)
    def _():
        send_ahead.start()

    @pl.when(jnp.logical_not(inner))
    def _():
        tell(known_sem.at[0], {"sp": inward})

    @pl.when(side == 1)
    def _():
        tell(known_sem.at[0], {"sp": me - 1})

    @pl.when(core == 1)
    def _():
        tell(known_sem.at[0], {"tp": 1 - core})

    replies = has_outward.astype(jnp.int32) + 2 - side - core

    @pl.when(replies > 0)
    def _():
        pl.semaphore_wait(known_sem.at[0], replies)

    tell_neighbours(known_sem.at[1])
    pl.semaphore_wait(known_sem.at[1], neighbours)
    tell_neighbours(known_sem.at[2])

    def query_copy(owner):
        return pltpu.make_async_remote_copy(
            src_ref=query_in.at[me], dst_ref=query_in.at[me],
            send_sem=query_sent.at[owner], recv_sem=query_recv.at[me],
            device_id={"sp": owner}, device_id_type=MESH,
        )

    def gate_copy(owner):
        return pltpu.make_async_remote_copy(
            src_ref=gate_send.at[owner], dst_ref=gate_in.at[me],
            send_sem=gate_sent.at[owner], recv_sem=gate_recv.at[me],
            device_id={"sp": owner}, device_id_type=MESH,
        )

    def part_copy(owner):
        return pltpu.make_async_remote_copy(
            src_ref=part_send.at[owner], dst_ref=part_in.at[me],
            send_sem=part_sent.at[owner], recv_sem=part_recv.at[me],
            device_id={"sp": owner}, device_id_type=MESH,
        )

    def block_copy(owner, t, size=tile):
        return pltpu.make_async_remote_copy(
            src_ref=outgoing.at[owner, :, pl.ds(t * tile, size), :],
            dst_ref=kv.at[:, pl.ds(pl.multiple_of(me * count + t * tile, LANES), size), :],
            send_sem=send_sem.at[owner, t], recv_sem=recv_sem.at[me, t],
            device_id={"sp": owner}, device_id_type=MESH,
        )

    def both_sizes(t, short, act):
        if t == ahead_tile:
            @pl.when(short)
            def _():
                act(tile - ahead_rows)

            @pl.when(jnp.logical_not(short))
            def _():
                act(tile)
        else:
            act(tile)

    def block_own(t):
        return pltpu.make_async_copy(
            outgoing.at[me, :, pl.ds(t * tile, tile), :],
            kv.at[:, pl.ds(pl.multiple_of(me * count + t * tile, tile), tile), :],
            recv_sem.at[me, t],
        )

    def send_block(owner, t):
        @pl.when(owner != me)
        def _():
            both_sizes(t, inner & crosses(owner), lambda size: block_copy(owner, t, size).start())

        @pl.when(owner == me)
        def _():
            block_own(t).start()

    def own_gates(owner, span):
        return jnp.concatenate([gate_own[owner, h, :, span] for h in range(per_owner)], axis=0)

    low = lax.broadcasted_iota(jnp.int32, (tile, LANES), 1) < head

    def open_links(first_round, last_round):
        for at in range(first_round - 1, last_round):
            pl.semaphore_wait(known_sem.at[at], neighbours)
            if at + 1 < layers:
                tell_neighbours(known_sem.at[at + 1])

    def send_queries():
        load_gates.wait()
        load_query.wait()
        query_in[me] = (query_own[...].astype(jnp.float32) * (head ** -0.5)).astype(jnp.bfloat16)

        @pl.loop(0, n - 1)
        def _(k):
            query_copy(partner(k, me, n)).start()

    def send_gates():
        @pl.loop(0, n - 1)
        def _(k):
            owner = partner(k, me, n)
            gate_send[owner] = own_gates(owner, slice(None)).astype(jnp.bfloat16)
            gate_copy(owner).start()

        gate_in[me] = own_gates(me, slice(None)).astype(jnp.bfloat16)

    head_row = lax.broadcasted_iota(jnp.int32, (per_owner, LANES), 0)
    tile_row = lax.broadcasted_iota(jnp.int32, (per_owner, tile), 0)
    lane = lax.broadcasted_iota(jnp.int32, (per_owner, LANES), 1)

    def read_own(owner):
        @pl.when(owner != me)
        def _():
            pltpu.make_async_copy(query_in.at[owner], query_in.at[owner], query_recv.at[owner]).wait()

        asked = jnp.concatenate(
            [query_in[owner].astype(jnp.float32), jnp.zeros((per_owner, LANES - head), jnp.float32)], axis=1
        )
        queries = [
            jnp.where(head_row == h, asked, 0.0).astype(jnp.bfloat16) for h in range(per_owner)
        ]
        top = jnp.full((per_owner, 1), -1e30, jnp.float32)
        total = jnp.zeros((per_owner, 1), jnp.float32)
        weighted = jnp.zeros((per_owner, LANES), jnp.float32)
        for t in range(tiles):
            span = pl.ds(t * tile, tile)
            blocks = [outgoing[owner, h, span, :] for h in range(per_owner)]
            scores = None
            for h in range(per_owner):
                term = lax.dot_general(
                    queries[h], blocks[h], (((1,), (1,)), ((), ())), preferred_element_type=jnp.float32
                )
                scores = term if scores is None else scores + term
            scores = scores - own_gates(owner, span)
            new_top = jnp.maximum(top, jnp.max(scores, axis=1, keepdims=True))
            scale = jnp.exp(top - new_top)
            probs = jnp.exp(scores - new_top)
            total = total * scale + jnp.sum(probs, axis=1, keepdims=True)
            weighted = weighted * scale
            for h in range(per_owner):
                picked = jnp.where(tile_row == h, probs, 0.0).astype(jnp.bfloat16)
                weighted = weighted + jnp.dot(picked, blocks[h], preferred_element_type=jnp.float32)
            top = new_top
        level = top + jnp.log(total)
        first = level.astype(jnp.bfloat16).astype(jnp.float32)
        second = (level - first).astype(jnp.bfloat16).astype(jnp.float32)
        third = level - first - second
        words = jnp.where(lane == 0, first, jnp.where(lane == 1, second, third))
        part_send[owner] = jnp.where(lane < head, words, weighted / total).astype(jnp.bfloat16)

        @pl.when(owner != me)
        def _():
            part_copy(owner).start()

    def project(step, first, relays=False):
        group = group_of(step)

        if first:
            for ahead in range(1, min(3, groups)):
                load_weight(ahead, 0).start()
                load_weight(ahead, 1).start()
        else:
            @pl.when(step + 2 < groups)
            def _():
                load_weight(step + 2, 0).start()
                load_weight(step + 2, 1).start()

        load_weight(step, 0).wait()
        load_weight(step, 1).wait()

        def multiply(left, store):
            size = left.shape[0]
            keys = jnp.dot(left, weights[step, 0], preferred_element_type=jnp.float32)
            values = jnp.dot(left, weights[step, 1], preferred_element_type=jnp.float32)
            for pair in range(columns // LANES):
                span = slice(pair * LANES, (pair + 1) * LANES)
                k, v = keys[:, span], values[:, span]
                joined = (
                    jnp.where(low[:size], k, pltpu.roll(v, head, 1)),
                    jnp.where(low[:size], pltpu.roll(k, head, 1), v),
                )
                for half in range(2):
                    local = pair * 2 + half
                    store(
                        group * owners + local // per_owner, local % per_owner, joined[half].astype(jnp.bfloat16)
                    )

        for t in range(tiles):
            if first:
                load_rows(t).wait()

            def keep(owner, h, block):
                outgoing[owner, h, pl.ds(t * tile, tile), :] = block

            multiply(rows[pl.ds(t * tile, tile), :], keep)
            if first and t == 0:
                open_links(3, near + 1)

                @pl.when(inner)
                def _():
                    for j in range(owners):
                        send_block(group * owners + j, t)

                open_links(near + 2, layers)

                @pl.when(jnp.logical_not(inner))
                def _():
                    for j in range(owners):
                        send_block(group * owners + j, t)
            elif t < early:
                for j in range(owners):
                    send_block(group * owners + j, t)
            if first and t == 0:
                send_queries()
        for j in range(owners):
            read_own(group * owners + j)
        if relays:
            @pl.when(inner)
            def _():
                def keep(owner, h, block):
                    relayed[owner, h] = block

                multiply(row_in[...], keep)
                for j in range(owners):
                    owner = group * owners + j

                    @pl.when(owner != me)
                    def _():
                        relay_copy(owner).start()

                    @pl.when(owner == me)
                    def _():
                        kv[:, mate_rows, :] = relayed[owner]

    mate_rows = pl.ds(pl.multiple_of(mate * count + ahead_at, 16), ahead_rows)

    def relay_copy(owner):
        return pltpu.make_async_remote_copy(
            src_ref=relayed.at[owner], dst_ref=kv.at[:, mate_rows, :],
            send_sem=relay_sent.at[owner], recv_sem=relay_recv.at[me],
            device_id={"sp": owner}, device_id_type=MESH,
        )

    project(0, True)
    send_gates()

    def across(step, carry):
        project(step, False)
        return carry

    lax.fori_loop(1, groups // 2, across, 0)

    @pl.when(inner)
    def _():
        send_ahead.wait()

    def along(step, carry):
        project(step, False, True)
        return carry

    lax.fori_loop(groups // 2, groups, along, 0)

    if early < tiles:
        @pl.when(core == 0)
        def _():
            @pl.loop(0, n)
            def _(k):
                for t in range(early, tiles):
                    send_block(partner(k, me, n), t)

    @pl.loop(0, n - 1)
    def _(k):
        source = partner(k, me, n)
        gate_copy(source).wait_send()
        query_copy(source).wait_send()
        pltpu.make_async_copy(gate_in.at[source], gate_in.at[source], gate_recv.at[source]).wait()

    for source in range(n):
        gate_out[:, source * count:(source + 1) * count] = gate_in[source].astype(jnp.float32)

    def merge(one, two):
        top_one, top_two = one[:, :1], two[:, :1]
        joint = jnp.maximum(top_one, top_two)
        both = one * jnp.exp(top_one - joint) + two * jnp.exp(top_two - joint)
        return jnp.where(lane < head // 2, joint, both)

    def unpack(part):
        words = part.astype(jnp.float32)
        level = words[:, 0:1] + words[:, 1:2] + words[:, 2:3]
        return jnp.where(lane < head // 2, level, jnp.where(lane < head, 1.0, words))

    def gather(k, carry):
        source = partner(n - 2 - k, me, n)
        part_copy(source).wait_send()
        pltpu.make_async_copy(part_in.at[source], part_in.at[source], part_recv.at[source]).wait()
        return merge(carry, unpack(part_in[source]))

    packed = lax.fori_loop(0, n - 1, gather, unpack(part_send[me]))
    mine[...] = packed
    swap = pltpu.make_async_remote_copy(
        src_ref=mine, dst_ref=theirs, send_sem=pair_sem.at[0], recv_sem=pair_sem.at[1],
        device_id={"tp": 1 - core}, device_id_type=MESH,
    )
    swap.start()
    swap.wait()
    other = theirs[...]
    joint = merge(jnp.where(core == 0, packed, other), jnp.where(core == 0, other, packed))
    at = head // 2
    answer = joint / joint[:, at:at + 1]
    read[...] = pltpu.roll(answer, head, 1)[:, :head].astype(jnp.bfloat16)

    def settle(t):
        block_own(t).wait()

        @pl.loop(0, n - 1)
        def _(k):
            source = partner(n - 2 - k, me, n)
            both_sizes(t, inner & crosses(source), lambda size: block_copy(source, t, size).wait_send())

            def arrived(size):
                span = pl.ds(t * tile, size)
                pltpu.make_async_copy(kv.at[:, span, :], kv.at[:, span, :], recv_sem.at[source, t]).wait()

            both_sizes(t, is_inner(source) & crosses(source), arrived)

    first_inner = jnp.where(right, near, near - 1) * 2

    @pl.loop(0, 2)
    def _(k):
        source = first_inner + k

        @pl.when(source != me)
        def _():
            pltpu.make_async_copy(
                kv.at[:, ahead_span, :], kv.at[:, ahead_span, :], relay_recv.at[source]
            ).wait()

    @pl.when(inner)
    def _():
        @pl.loop(0, n // 2)
        def _(k):
            owner = jnp.where(right, n // 2, 0) + k

            @pl.when(owner != me)
            def _():
                relay_copy(owner).wait_send()

    for t in range(early):
        settle(t)
    if early < tiles:
        @pl.when(core == 0)
        def _():
            for t in range(early, tiles):
                settle(t)


def rest_kernel(
    n, first_row,
    outgoing, after,
    late,
    send_sem, recv_sem,
):
    me = lax.axis_index("sp")
    size = outgoing.shape[2] - first_row
    held = pl.ds(first_row, size)

    def rows_of(source):
        return pl.ds(pl.multiple_of(source * size, size), size)

    def block_copy(owner):
        return pltpu.make_async_remote_copy(
            src_ref=outgoing.at[owner, :, held, :], dst_ref=late.at[:, rows_of(me), :],
            send_sem=send_sem.at[owner], recv_sem=recv_sem.at[me],
            device_id={"sp": owner}, device_id_type=MESH,
        )

    @pl.when(lax.axis_index("tp") == 1)
    def _():
        barrier = pltpu.get_barrier_semaphore()

        @pl.loop(1, n)
        def _(k):
            pl.semaphore_signal(
                barrier, inc=1, device_id={"sp": lax.rem(me + k, n)}, device_id_type=MESH
            )

        pl.semaphore_wait(barrier, n - 1)

        @pl.loop(0, n - 1)
        def _(k):
            block_copy(partner(k, me, n, 1)).start()

        late[:, rows_of(me), :] = outgoing[me, :, held, :]

        @pl.loop(0, n - 1)
        def _(k):
            source = partner(n - 2 - k, me, n)
            block_copy(source).wait_send()
            pltpu.make_async_copy(
                outgoing.at[0, :, held, :], late.at[:, rows_of(source), :], recv_sem.at[source]
            ).wait()


def finish_kernel(n, first_row, kv, gates, answer, kv_out, gate_out, read, after, sem):
    count = kv.shape[1] // n

    def part(source, start, size, at):
        span = pl.ds(source * count + start, size)
        return pltpu.make_async_copy(kv.at[:, span, :], kv_out.at[:, span, :], sem.at[at])

    small = [
        pltpu.make_async_copy(gates, gate_out, sem.at[2 * n]),
        pltpu.make_async_copy(answer, read, sem.at[2 * n + 1]),
    ]
    early = [part(source, 0, first_row, source) for source in range(n)]
    for copy in early + small:
        copy.start()
    after[...] = jnp.zeros_like(after)
    if first_row < count:
        @pl.when(lax.axis_index("tp") == 0)
        def _():
            late = [part(source, first_row, count - first_row, n + source) for source in range(n)]
            for copy in late:
                copy.start()
            for copy in late:
                copy.wait()
    for copy in early + small:
        copy.wait()


def last_kernel(n, first_row, late, kv, kv_out, sem):
    count = kv_out.shape[1] // n
    size = count - first_row

    @pl.when(lax.axis_index("tp") == 1)
    def _():
        copies = [
            pltpu.make_async_copy(
                late.at[:, pl.ds(source * size, size), :],
                kv_out.at[:, pl.ds(source * count + first_row, size), :],
                sem.at[source],
            )
            for source in range(n)
        ]
        for copy in copies:
            copy.start()
        for copy in copies:
            copy.wait()


def on_device(n, tokens, key_weight, value_weight, cum_gate, query):
    _, _, count, width = tokens.shape
    heads = cum_gate.shape[1]
    per_owner, head = query.shape[1], query.shape[2]
    tile = 256 if count % 256 == 0 else count
    columns = max(per_owner * head, LANES)
    groups = heads * head // columns
    tiles = count // tile
    ahead_rows = tile // 8
    any_space = pl.BlockSpec(memory_space=pl.ANY)
    outside = pl.BlockSpec(memory_space=pltpu.HBM)
    vmem = pl.BlockSpec(memory_space=pltpu.VMEM)
    kv, outgoing, gates, answer = pl.pallas_call(
        functools.partial(exchange_kernel, n, per_owner, tile, head, ahead_rows),
        name="exchange",
        out_shape=(
            pltpu.VMEM((per_owner, n * count, 2 * head), jnp.bfloat16),
            pltpu.VMEM((n, per_owner, count, 2 * head), jnp.bfloat16),
            pltpu.VMEM((per_owner, n * count), jnp.float32),
            pltpu.VMEM((per_owner, head), jnp.bfloat16),
        ),
        in_specs=[outside] * 5,
        out_specs=(vmem, vmem, vmem, vmem),
        scratch_shapes=[
            pltpu.VMEM((count, width), jnp.bfloat16),
            pltpu.VMEM((groups, 2, width, columns), jnp.bfloat16),
            pltpu.VMEM((n, per_owner, 1, count), jnp.float32),
            pltpu.VMEM((n, per_owner, count), jnp.bfloat16),
            pltpu.VMEM((n, per_owner, count), jnp.bfloat16),
            pltpu.VMEM((per_owner, head), jnp.bfloat16),
            pltpu.VMEM((n, per_owner, head), jnp.bfloat16),
            pltpu.VMEM((n, per_owner, LANES), jnp.bfloat16),
            pltpu.VMEM((n, per_owner, LANES), jnp.bfloat16),
            pltpu.VMEM((per_owner, LANES), jnp.float32),
            pltpu.VMEM((per_owner, LANES), jnp.float32),
            pltpu.VMEM((ahead_rows, width), jnp.bfloat16),
            pltpu.VMEM((n, per_owner, ahead_rows, 2 * head), jnp.bfloat16),
            pltpu.SemaphoreType.DMA((tiles,)),
            pltpu.SemaphoreType.DMA((groups, 2)),
            pltpu.SemaphoreType.DMA((3,)),
            pltpu.SemaphoreType.DMA((n, tiles)),
            pltpu.SemaphoreType.DMA((n, tiles)),
            pltpu.SemaphoreType.REGULAR((n // 2,)),
            pltpu.SemaphoreType.DMA((2,)),
            pltpu.SemaphoreType.DMA((n,)),
            pltpu.SemaphoreType.DMA((n,)),
            pltpu.SemaphoreType.DMA((n,)),
            pltpu.SemaphoreType.DMA((n,)),
            pltpu.SemaphoreType.DMA((n,)),
            pltpu.SemaphoreType.DMA((n,)),
            pltpu.SemaphoreType.DMA((n,)),
            pltpu.SemaphoreType.DMA((n,)),
            pltpu.SemaphoreType.DMA((2,)),
        ],
        compiler_params=pltpu.CompilerParams(
            collective_id=0, has_side_effects=True, vmem_limit_bytes=48 * 1024 * 1024
        ),
    )(
        tokens.reshape(count, width),
        key_weight,
        value_weight,
        cum_gate.reshape(n, per_owner, 1, count),
        query.reshape(per_owner, head),
    )
    first_row = max(tiles - 1, 1) * tile
    whole = jax.ShapeDtypeStruct((per_owner, n * count, 2 * head), jnp.bfloat16)
    kv_out, gate_out, read, after = pl.pallas_call(
        functools.partial(finish_kernel, n, first_row),
        name="finish",
        out_shape=(
            whole,
            jax.ShapeDtypeStruct((per_owner, n * count), jnp.float32),
            jax.ShapeDtypeStruct((per_owner, head), jnp.bfloat16),
            pltpu.VMEM((8, LANES), jnp.float32),
        ),
        in_specs=[vmem, vmem, vmem],
        out_specs=(any_space, any_space, any_space, vmem),
        scratch_shapes=[pltpu.SemaphoreType.DMA((2 * n + 2,))],
        compiler_params=pltpu.CompilerParams(vmem_limit_bytes=16 * 1024 * 1024),
    )(kv, gates, answer)
    if first_row < count:
        late = pl.pallas_call(
            functools.partial(rest_kernel, n, first_row),
            name="rest",
            out_shape=pltpu.VMEM((per_owner, n * (count - first_row), 2 * head), jnp.bfloat16),
            in_specs=[vmem, vmem],
            out_specs=vmem,
            scratch_shapes=[pltpu.SemaphoreType.DMA((n,)), pltpu.SemaphoreType.DMA((n,))],
            compiler_params=pltpu.CompilerParams(
                collective_id=1, has_side_effects=True, vmem_limit_bytes=16 * 1024 * 1024
            ),
        )(outgoing, after)
        kv_out = pl.pallas_call(
            functools.partial(last_kernel, n, first_row),
            name="last",
            out_shape=whole,
            in_specs=[vmem, any_space],
            out_specs=any_space,
            input_output_aliases={1: 0},
            scratch_shapes=[pltpu.SemaphoreType.DMA((n,))],
            compiler_params=pltpu.CompilerParams(vmem_limit_bytes=16 * 1024 * 1024),
        )(late, kv_out)
    return kv_out[None], gate_out[None], read[None]


def solution(mesh):
    placed = (P("gr", "tp", "sp", None), P(), P(), P("gr", None, "tp", "sp"), P("gr", "sp", None))
    return jax.shard_map(
        functools.partial(on_device, mesh.shape["sp"]),
        mesh=mesh,
        in_specs=placed,
        out_specs=(P("gr", "sp", "tp", None), P("gr", "sp", "tp"), P("gr", "sp", None)),
        check_vma=False,
    )
```
